32 devices in a mesh: fs: 8 (over z, y), tp: 4 (over x, core).
Axes of the slice: x: 2, y: 2, z: 4, core: 2. Of those that a mesh axis runs over, the one named last changes fastest.
Arguments:
- later_gate: bfloat16 [5120, 5632], P('fs', 'tp'), may hold values from -6 to 6
- later_up: bfloat16 [5120, 5632], P('fs', 'tp'), may hold values from -6 to 6
- early_gate: bfloat16 [5120, 5632], P('fs', 'tp'), may hold values from -6 to 6
- early_up: bfloat16 [5120, 5632], P('fs', 'tp'), may hold values from -6 to 6
- early_cotangent: bfloat16 [5120, 2048], P(('fs', 'tp')), may hold values from -6 to 6
- down_weight: bfloat16 [5632, 2048], P('tp', 'fs'), may hold values from -0.078125 to 0.078125
- grad_running: float32 [5632, 2048], P('tp', 'fs'), may hold values from -224 to 224
Outputs:
- mixed: bfloat16 [5120, 2048], P(('fs', 'tp'))
- gate_grad: bfloat16 [5120, 5632], P('fs', 'tp')
- up_grad: bfloat16 [5120, 5632], P('fs', 'tp')
- grad_total: float32 [5632, 2048], P('tp', 'fs')
The draws below stay inside these ranges and needn't reach their ends.
All inputs are finite; a program needn't handle non-finite values.
Results may differ from the reference program's by a relative error of at most 0.009.
Values may be sent and summed in bfloat16 or wider, within the bound.
A program may use at most 128 MiB of HBM per device.

```python
import jax
import jax.numpy as jnp

D = 2048
FF = 5632
TOKENS = 5120
N_TP = 4


def raised(entries, own_key, source, target, shards_of, factor):
    owner, partner = [(jnp.arange(entries.shape[dim]) // (entries.shape[dim] // shards_of)).reshape([-1 if axis == dim else 1 for axis in range(entries.ndim)]) for dim in (source, target)]
    chosen = jax.random.permutation(own_key, shards_of)[partner]
    strong = (owner == chosen) | (owner == (partner + shards_of // 2) % shards_of)
    return jnp.where(strong, factor * entries, entries)


def steps_of(rng, extent, pieces, least, top_value):
    factor_of, own = 1.0, jax.random.fold_in(rng, 6)
    for axis_at, shards_of in pieces:
        steps = jnp.exp(jax.random.uniform(jax.random.fold_in(own, axis_at), (shards_of,), jnp.float32, least / len(pieces), top_value / len(pieces)))
        factor_of = factor_of * jnp.repeat(steps, extent[axis_at] // shards_of).reshape([-1 if axis == axis_at else 1 for axis in range(len(extent))])
    return factor_of


def centred(rng, shape, width, reach, shards=(), kind=jnp.bfloat16):
    values = jax.random.normal(rng, shape, jnp.float32) * width
    if len(shards) > 0:
        values = steps_of(rng, shape, shards, -0.22, 0.18) * values
    return jnp.clip(values, min=-reach, max=reach).astype(kind)


def bell_draw_with(own_key, shape, spread, most, cuts, heavy, dtype=jnp.bfloat16):
    drawn = spread * jax.random.normal(own_key, shape, jnp.float32)
    if cuts:
        drawn = drawn * steps_of(own_key, shape, cuts, -0.22, 0.18)
    return jnp.clip(raised(drawn, jax.random.fold_in(own_key, 3), *heavy), -most, most).astype(dtype)


def setup_inputs(seed: int = 0) -> dict:
    key_list = jax.random.split(jax.random.key(seed), 8)
    return {
        "later_gate": centred(key_list[0], (TOKENS, FF), 1.0, 6.0, ((0, 8), (1, 4))),
        "later_up": centred(key_list[1], (TOKENS, FF), 1.0, 6.0, ((0, 8), (1, 4))),
        "early_gate": centred(key_list[2], (TOKENS, FF), 1.0, 6.0, ((0, 8), (1, 4))),
        "early_up": centred(key_list[3], (TOKENS, FF), 1.0, 6.0, ((0, 8), (1, 4))),
        "early_cotangent": bell_draw_with(key_list[4], (TOKENS, D), 1.0, 6.0, ((0, 32),), (0, 1, 32, 2.75)),
        "down_weight": centred(key_list[5], (FF, D), FF ** -0.5, 0.078125, ((0, 4), (1, 8))),
        "grad_running": centred(key_list[6], (FF, D), (0.5 * TOKENS ** 0.5), 224.0, ((0, 4), (1, 8)), jnp.float32),
    }


def reference(later_gate, later_up, early_gate, early_up, early_cotangent, down_weight, grad_running):
    later_hidden = (jax.nn.silu(later_gate.astype(jnp.float32)) * later_up.astype(jnp.float32)).astype(jnp.bfloat16)
    block = FF // N_TP
    total = jnp.zeros((later_hidden.shape[0], D), jnp.float32)
    for index in range(N_TP):
        part = jnp.dot(later_hidden[:, index * block:(index + 1) * block], down_weight[index * block:(index + 1) * block], preferred_element_type=jnp.float32)
        total = total + part.astype(jnp.bfloat16).astype(jnp.float32)
    mixed = total.astype(jnp.bfloat16)
    gate_value = early_gate.astype(jnp.float32)
    up_value = early_up.astype(jnp.float32)
    sigma = jax.nn.sigmoid(gate_value)
    early_hidden = (gate_value * sigma * up_value).astype(jnp.bfloat16)
    hidden_cot = jnp.dot(early_cotangent, down_weight.T, preferred_element_type=jnp.float32)
    gate_grad = (hidden_cot * up_value * sigma * (1.0 + gate_value * (1.0 - sigma))).astype(jnp.bfloat16)
    up_grad = (hidden_cot * gate_value * sigma).astype(jnp.bfloat16)
    grad_total = grad_running + jnp.dot(early_hidden.T, early_cotangent, preferred_element_type=jnp.float32)
    return (mixed, gate_grad, up_grad, grad_total)
```

```python
import functools

import jax
import jax.numpy as jnp
from jax import lax
from jax.experimental import pallas as pl
from jax.experimental.pallas import tpu as pltpu
from jax.sharding import PartitionSpec as P

PAIR = 2
F32, BF16 = jnp.float32, jnp.bfloat16


def by_collectives(
    later_gate, later_up, early_gate, early_up, early_cotangent, down_weight, grad_running
):
    later_hidden = (
        jax.nn.silu(later_gate.astype(F32)) * later_up.astype(F32)
    ).astype(BF16)
    gate_value = early_gate.astype(F32)
    up_value = early_up.astype(F32)
    sigma = jax.nn.sigmoid(gate_value)
    early_hidden = (gate_value * sigma * up_value).astype(BF16)
    cot_rows = lax.all_gather(early_cotangent, "tp", axis=0, tiled=True)
    whole = lax.all_gather(down_weight, "fs", axis=1, tiled=True)
    mixed = lax.psum_scatter(
        jnp.dot(later_hidden, whole, preferred_element_type=F32).astype(BF16),
        "tp",
        scatter_dimension=0,
        tiled=True,
    )
    hidden_cot = lax.dot_general(
        cot_rows, whole, (((1,), (1,)), ((), ())), preferred_element_type=F32
    )
    gate_grad = (hidden_cot * up_value * sigma * (1.0 + gate_value * (1.0 - sigma))).astype(BF16)
    up_grad = (hidden_cot * gate_value * sigma).astype(BF16)
    summed = lax.psum_scatter(
        lax.dot_general(
            cot_rows, early_hidden, (((0,), (0,)), ((), ())), preferred_element_type=F32
        ),
        "fs",
        scatter_dimension=0,
        tiled=True,
    )
    return (mixed, gate_grad, up_grad, grad_running + summed.T)


def parts_of(K):
    size = -(-(K // 128) // 4) * 128
    return [(a, min(a + size, K)) for a in range(0, K, size)]


def kernel(
    fs, n,
    lg_ref, lu_ref, eg_ref, eu_ref, cot_ref, w_ref, gr_ref,
    mixed_ref, gg_ref, ug_ref, gt_ref,
    lg, lu, eg, eu, run, W, C, Cp, He, Hl, Gs, Gr, own_g, Ms, Mr, hc,
    loc, wup_s, wdn_s, wy_s, w_r, c_s, c_r, cy_s, cy_r, cp_s, cp_r, h_s, h_r, g_s, g_r, m_s, m_r,
    wb_s, wb_r, wbu_s, wbd_s,
):
    Z = fs // PAIR
    T, K = lg.shape
    B = W.shape[2]
    R = T // n
    early = max(K * 3 // 22 // 64, 1) * 64
    me_f, me = lax.axis_index("fs"), lax.axis_index("tp")
    z, y = me_f // PAIR, me_f % PAIR
    buddy = {"fs": z * PAIR + 1 - y}

    def remote(src, dst, ss, rs, to):
        return pltpu.make_async_remote_copy(
            src_ref=src, dst_ref=dst, send_sem=ss, recv_sem=rs,
            device_id=to, device_id_type=pl.DeviceIdType.MESH,
        )

    def block(f):
        return pl.ds(pl.multiple_of(f * B, B), B)

    def rows(t):
        return pl.ds(pl.multiple_of(t * R, R), R)

    others_z = [lax.rem(z + k, Z) for k in range(1, Z)]
    others_t = [lax.rem(me + k, n) for k in range(1, n)]

    loads = [
        pltpu.make_async_copy(src, dst, loc.at[i])
        for i, (src, dst) in enumerate((
            (w_ref, W.at[me_f]), (cot_ref, C.at[rows(me), :]), (eg_ref, eg), (eu_ref, eu),
            (lg_ref, lg), (lu_ref, lu), (gr_ref, run),
        ))
    ]
    for copy in loads:
        copy.start()

    barrier = pltpu.get_barrier_semaphore()
    for to in [buddy] + [{"fs": k * PAIR + y} for k in others_z] + [{"tp": t} for t in others_t]:
        pl.semaphore_signal(barrier, inc=1, device_id=to, device_id_type=pl.DeviceIdType.MESH)
    pl.semaphore_wait(barrier, 1 + len(others_z) + len(others_t))

    def up(zz):
        f = zz * PAIR + y
        return remote(W.at[f], W.at[f], wup_s.at[zz], w_r.at[f], {"fs": (z + 1) * PAIR + y})

    def down(zz):
        f = zz * PAIR + y
        return remote(W.at[f], W.at[f], wdn_s.at[zz], w_r.at[f], {"fs": (z - 1) * PAIR + y})

    def across(zz, source=y):
        f = zz * PAIR + source
        part = W.at[f, early:, :]
        return remote(part, part, wy_s.at[zz], w_r.at[f], buddy)

    def first_across():
        part = W.at[me_f, :early, :]
        return remote(part, part, wb_s.at[0], wb_r.at[z], buddy)

    def first_up(zz):
        part = W.at[zz * PAIR + 1 - y, :early, :]
        return remote(part, part, wbu_s.at[zz], wb_r.at[zz], {"fs": (z + 1) * PAIR + y})

    def first_down(zz):
        part = W.at[zz * PAIR + 1 - y, :early, :]
        return remote(part, part, wbd_s.at[zz], wb_r.at[zz], {"fs": (z - 1) * PAIR + y})

    def got_w(f):
        remote(W.at[f], W.at[f], wy_s.at[0], w_r.at[f], buddy).wait_recv()

    loads[0].wait()

    @pl.when(z < Z - 1)
    def _():
        up(z).start()

    @pl.when(z > 0)
    def _():
        down(z).start()

    first_across().start()
    loads[1].wait()
    cy = [
        remote(
            C.at[rows(me), block(k * PAIR + 1 - y)], Cp.at[rows(me), pl.ds(k * B, B)],
            cy_s.at[k], cy_r.at[k], buddy,
        )
        for k in range(Z)
    ]
    for copy in cy:
        copy.start()

    def c_copy(t, f, source):
        part = C.at[rows(source), block(f)]
        return remote(part, part, c_s.at[t * fs + f], c_r.at[source * fs + f], {"tp": t})

    def c_send(side):
        for k in range(Z):
            for t in others_t:
                c_copy(t, k * PAIR + side, me).start()

    def c_wait(side):
        for k in range(Z):
            for t in others_t:
                c_copy(t, k * PAIR + side, t).wait_recv()

    c_send(y)
    step = 32 if T % 32 == 0 else R

    def hidden(g_ref, u_ref, out, a, b):
        @pl.loop(0, T // step)
        def _(i):
            at = pl.ds(pl.multiple_of(i * step, step), step)
            g = g_ref[at, a:b].astype(F32)
            out[at, a:b] = (g * jax.nn.sigmoid(g) * u_ref[at, a:b].astype(F32)).astype(BF16)

    loads[2].wait()
    loads[3].wait()
    swaps = []
    for q, (a, b) in enumerate(parts_of(K)):
        hidden(eg, eu, He.at[0], a, b)
        swaps.append(
            remote(He.at[0, :, a:b], He.at[1, :, a:b], h_s.at[q], h_r.at[q], buddy)
        )
        swaps[-1].start()

    for copy in cy:
        copy.wait_recv()
    for t in others_t:
        remote(Cp.at[rows(me), :], Cp.at[rows(me), :], cp_s.at[t], cp_r.at[me], {"tp": t}).start()
    c_send(1 - y)

    loads[4].wait()
    loads[5].wait()
    hidden(lg, lu, Hl, 0, K)

    def m_copy(f, t):
        return remote(
            Ms.at[rows(t), block(f)], Mr.at[me, :, block(f)],
            m_s.at[f * n + t], m_r.at[f * n + me], {"tp": t},
        )

    def mix(f):
        @pl.loop(0, n)
        def _(t):
            part = jnp.dot(Hl[rows(t), :], W[f], preferred_element_type=F32)
            Ms[rows(t), block(f)] = part.astype(BF16)

        for t in others_t:
            m_copy(f, t).start()

    cuts = [(a, min(a + 512, K)) for a in range(0, K, 512)]

    def back(f, first):
        @pl.loop(0, n)
        def _(t):
            c = C[rows(t), block(f)]
            for a, b in cuts:
                term = lax.dot_general(
                    c, W[f, a:b, :], (((1,), (1,)), ((), ())), preferred_element_type=F32
                )
                hc[rows(t), a:b] = term if first else hc[rows(t), a:b] + term

    def in_order(body, first=0, end=2 * Z - 1):
        @pl.loop(first, end)
        def _(c):
            d = (c + 1) // 2
            zz = jnp.where(c % 2 == 1, z - d, z + d)

            @pl.when((zz >= 0) & (zz < Z))
            def _():
                body(c, zz)

    def relay(c, zz):
        @pl.when(c > 0)
        def _():
            got_w(zz * PAIR + y)

        @pl.when((c > 0) & (zz < z) & (z < Z - 1))
        def _():
            up(zz).start()

        @pl.when((c > 0) & (zz > z) & (z > 0))
        def _():
            down(zz).start()

        part = W.at[zz * PAIR + 1 - y, :early, :]
        remote(part, part, wb_s.at[0], wb_r.at[zz], buddy).wait_recv()

        @pl.when((zz <= z) & (z < Z - 1))
        def _():
            first_up(zz).start()

        @pl.when((zz >= z) & (z > 0))
        def _():
            first_down(zz).start()

        across(zz).start()
        mix(zz * PAIR + y)

    over_rows = (((0,), (0,)), ((), ()))

    def g_copy(q, zz, source):
        a, b = parts_of(K)[q]
        return remote(
            Gs.at[zz, a:b, :], Gr.at[source, a:b, :],
            g_s.at[q * Z + zz], g_r.at[q * Z + source], {"fs": zz * PAIR + y},
        )

    def terms(q):
        swaps[q].wait_recv()
        a, b = parts_of(K)[q]

        @pl.loop(a // 128, b // 128)
        def _(i):
            at = pl.ds(pl.multiple_of(i * 128, 128), 128)
            mine, theirs = He[0, :, at], He[1, :, at]
            for k in range(Z):
                zz = lax.rem(z + k, Z)
                term = lax.dot_general(
                    mine, C[:, block(zz * PAIR + y)], over_rows, preferred_element_type=F32
                ) + lax.dot_general(theirs, Cp[:, block(zz)], over_rows, preferred_element_type=F32)
                if k == 0:
                    own_g[at, :] = term
                else:
                    Gs[zz, at, :] = term.astype(BF16)

        for zz in others_z:
            g_copy(q, zz, z).start()

    parts = len(parts_of(K))
    near = min(5, 2 * Z - 1)
    in_order(relay, 0, near)
    c_wait(y)
    for t in others_t:
        remote(Cp.at[rows(t), :], Cp.at[rows(t), :], cp_s.at[t], cp_r.at[t], {"tp": t}).wait_recv()
    for q in range(parts // 2):
        terms(q)
    in_order(relay, near)
    for q in range(parts // 2, parts):
        terms(q)
    c_wait(1 - y)

    back(z * PAIR + y, True)
    in_order(lambda c, zz: pl.when(c > 0)(lambda: back(zz * PAIR + y, False)))

    def partner(c, zz):
        f = zz * PAIR + 1 - y
        across(zz, 1 - y).wait_recv()
        mix(f)
        back(f, False)

    in_order(partner)

    for t in range(n):
        @pl.loop(t * R // step, (t + 1) * R // step)
        def _(i):
            at = pl.ds(pl.multiple_of(i * step, step), step)
            g, u, h = eg[at, :].astype(F32), eu[at, :].astype(F32), hc[at, :]
            s = jax.nn.sigmoid(g)
            gg_ref[at, :] = (h * u * s * (1.0 + g * (1.0 - s))).astype(BF16)
            ug_ref[at, :] = (h * g * s).astype(BF16)

    for q in range(parts):
        for zz in others_z:
            g_copy(q, zz, zz).wait_recv()
    loads[6].wait()

    @pl.loop(0, K // 128)
    def _(i):
        at = pl.ds(pl.multiple_of(i * 128, 128), 128)
        total = own_g[at, :]
        for zz in others_z:
            total = total + Gr[zz, at, :].astype(F32)
        gt_ref[at, :] = run[at, :] + total

    @pl.loop(0, fs)
    def _(f):
        for t in others_t:
            remote(
                Ms.at[rows(t), block(f)], Mr.at[t, :, block(f)],
                m_s.at[f * n + t], m_r.at[f * n + t], {"tp": t},
            ).wait_recv()
        total = Ms[rows(me), block(f)].astype(F32)
        for t in others_t:
            total = total + Mr[t, :, block(f)].astype(F32)
        mixed_ref[:, block(f)] = total.astype(BF16)

    def sent(c, zz):
        @pl.when((zz <= z) & (z < Z - 1))
        def _():
            up(zz).wait_send()
            first_up(zz).wait_send()

        @pl.when((zz >= z) & (z > 0))
        def _():
            down(zz).wait_send()
            first_down(zz).wait_send()

        across(zz).wait_send()

    in_order(sent)
    first_across().wait_send()
    for copy in cy:
        copy.wait_send()
    for t in others_t:
        for f in range(fs):
            c_copy(t, f, me).wait_send()
        remote(Cp.at[rows(me), :], Cp.at[rows(me), :], cp_s.at[t], cp_r.at[me], {"tp": t}).wait_send()
    for copy in swaps:
        copy.wait_send()
    for q in range(parts):
        for zz in others_z:
            g_copy(q, zz, z).wait_send()

    @pl.loop(0, fs)
    def _(f):
        for t in others_t:
            m_copy(f, t).wait_send()


def by_kernel(fs, n, *args):
    later_gate, cot, weight = args[0], args[4], args[5]
    T, K = later_gate.shape
    R, D = cot.shape
    B = weight.shape[1]
    Z = fs // PAIR
    parts = len(parts_of(K))
    sem = pltpu.SemaphoreType.DMA
    anywhere = pl.BlockSpec(memory_space=pl.ANY)
    return pl.pallas_call(
        functools.partial(kernel, fs, n),
        out_shape=(
            pltpu.VMEM((R, D), BF16),
            pltpu.VMEM((T, K), BF16),
            pltpu.VMEM((T, K), BF16),
            pltpu.VMEM((K, B), F32),
        ),
        in_specs=[anywhere] * 7,
        out_specs=(pl.BlockSpec(memory_space=pltpu.VMEM),) * 4,
        scratch_shapes=[
            pltpu.VMEM((T, K), BF16), pltpu.VMEM((T, K), BF16),
            pltpu.VMEM((T, K), BF16), pltpu.VMEM((T, K), BF16),
            pltpu.VMEM((K, B), F32),
            pltpu.VMEM((fs, K, B), BF16),
            pltpu.VMEM((T, D), BF16),
            pltpu.VMEM((T, Z * B), BF16),
            pltpu.VMEM((2, T, K), BF16),
            pltpu.VMEM((T, K), BF16),
            pltpu.VMEM((Z, K, B), BF16), pltpu.VMEM((Z, K, B), BF16),
            pltpu.VMEM((K, B), F32),
            pltpu.VMEM((T, D), BF16),
            pltpu.VMEM((n, R, D), BF16),
            pltpu.VMEM((T, K), F32),
            sem((7,)),
            sem((Z,)), sem((Z,)), sem((Z,)), sem((fs,)),
            sem((n * fs,)), sem((n * fs,)), sem((Z,)), sem((Z,)), sem((n,)), sem((n,)),
            sem((parts,)), sem((parts,)), sem((parts * Z,)), sem((parts * Z,)),
            sem((fs * n,)), sem((fs * n,)),
            sem((1,)), sem((Z,)), sem((Z,)), sem((Z,)),
        ],
        compiler_params=pltpu.CompilerParams(
            collective_id=0, has_side_effects=True, vmem_limit_bytes=52 * 2**20
        ),
    )(*args)


def solution(mesh):
    fs, n = mesh.shape["fs"], mesh.shape["tp"]

    def on_device(*args):
        T, K = args[0].shape
        B = args[5].shape[1]
        if fs % PAIR == 0 and fs >= 4 and B % 128 == 0 and K % 128 == 0 and (T // n) % 32 == 0:
            return by_kernel(fs, n, *args)
        return by_collectives(*args)

    placed = (
        P("fs", "tp"),
        P("fs", "tp"),
        P("fs", "tp"),
        P("fs", "tp"),
        P(("fs", "tp"), None),
        P("tp", "fs"),
        P("tp", "fs"),
    )
    return jax.shard_map(
        on_device,
        mesh=mesh,
        in_specs=placed,
        out_specs=(P(("fs", "tp"), None), P("fs", "tp"), P("fs", "tp"), P("tp", "fs")),
        check_vma=False,
    )
```

```python
import functools

import jax
import jax.numpy as jnp
from jax import lax
from jax.experimental import pallas as pl
from jax.experimental.pallas import tpu as pltpu
from jax.sharding import PartitionSpec as P

PAIR = 2
F32, BF16 = jnp.float32, jnp.bfloat16


def by_collectives(
    later_gate, later_up, early_gate, early_up, early_cotangent, down_weight, grad_running
):
    later_hidden = (
        jax.nn.silu(later_gate.astype(F32)) * later_up.astype(F32)
    ).astype(BF16)
    gate_value = early_gate.astype(F32)
    up_value = early_up.astype(F32)
    sigma = jax.nn.sigmoid(gate_value)
    early_hidden = (gate_value * sigma * up_value).astype(BF16)
    cot_rows = lax.all_gather(early_cotangent, "tp", axis=0, tiled=True)
    whole = lax.all_gather(down_weight, "fs", axis=1, tiled=True)
    mixed = lax.psum_scatter(
        jnp.dot(later_hidden, whole, preferred_element_type=F32).astype(BF16),
        "tp",
        scatter_dimension=0,
        tiled=True,
    )
    hidden_cot = lax.dot_general(
        cot_rows, whole, (((1,), (1,)), ((), ())), preferred_element_type=F32
    )
    gate_grad = (hidden_cot * up_value * sigma * (1.0 + gate_value * (1.0 - sigma))).astype(BF16)
    up_grad = (hidden_cot * gate_value * sigma).astype(BF16)
    summed = lax.psum_scatter(
        lax.dot_general(
            cot_rows, early_hidden, (((0,), (0,)), ((), ())), preferred_element_type=F32
        ),
        "fs",
        scatter_dimension=0,
        tiled=True,
    )
    return (mixed, gate_grad, up_grad, grad_running + summed.T)


def cuts_of(a, b, size=256):
    return [(k, min(k + size, b)) for k in range(a, b, size)]


def kernel(
    fs, n,
    lg_ref, lu_ref, eg_ref, eu_ref, cot_ref, w_ref, gr_ref,
    mixed_ref, gg_ref, ug_ref, gt_ref,
    lg, lu, eg, eu, W, C, Cp, He, Hl, Gs, Gr, Ms, Mr, hc,
    loc, wu_s, wd_s, w_r, bu_s, bd_s, by_s, b_r, la_s, la_r, lb_s, lb_r,
    c_s, c_r, cy_s, cy_r, cp_s, cp_r, h_s, h_r, g_s, g_r, m_s, m_r,
):
    Z = fs // PAIR
    T, K = lg.shape
    B = W.shape[2]
    R = T // n
    early = max(K // 2 // 64, 1) * 64
    split = max((early + K) // 2 // 256 * 256, early)
    ready = early // 256 * 256
    parts = cuts_of(0, K)
    me_f, me = lax.axis_index("fs"), lax.axis_index("tp")
    z, y = me_f // PAIR, me_f % PAIR
    buddy = {"fs": z * PAIR + 1 - y}
    above, below = {"fs": (z + 1) * PAIR + y}, {"fs": (z - 1) * PAIR + y}
    has_above, has_below = z < Z - 1, z > 0

    def remote(src, dst, ss, rs, to):
        return pltpu.make_async_remote_copy(
            src_ref=src, dst_ref=dst, send_sem=ss, recv_sem=rs,
            device_id=to, device_id_type=pl.DeviceIdType.MESH,
        )

    def block(f):
        return pl.ds(pl.multiple_of(f * B, B), B)

    def rows(t):
        return pl.ds(pl.multiple_of(t * R, R), R)

    others_t = [lax.rem(me + k, n) for k in range(1, n)]

    loads = [
        pltpu.make_async_copy(src, dst, loc.at[i])
        for i, (src, dst) in enumerate((
            (w_ref, W.at[me_f]), (cot_ref, C.at[rows(me), :]), (eg_ref, eg), (eu_ref, eu),
            (lg_ref, lg), (lu_ref, lu), (gr_ref, gt_ref),
        ))
    ]
    for copy in loads:
        copy.start()

    barrier = pltpu.get_barrier_semaphore()

    def greet(to):
        pl.semaphore_signal(barrier, inc=1, device_id=to, device_id_type=pl.DeviceIdType.MESH)

    pl.when(has_above)(lambda: greet(above))
    pl.when(has_below)(lambda: greet(below))
    for to in [buddy] + [{"tp": t} for t in others_t]:
        greet(to)
    pl.semaphore_wait(barrier, n + has_above.astype(jnp.int32) + has_below.astype(jnp.int32))

    def up(zz):
        f = zz * PAIR + y
        return remote(W.at[f], W.at[f], wu_s.at[zz], w_r.at[zz], above)

    def down(zz):
        f = zz * PAIR + y
        return remote(W.at[f], W.at[f], wd_s.at[zz], w_r.at[zz], below)

    def early_part(zz, side):
        return W.at[zz * PAIR + side, :early, :]

    def early_across():
        part = early_part(z, y)
        return remote(part, part, by_s.at[0], b_r.at[z], buddy)

    def early_up(zz):
        part = early_part(zz, 1 - y)
        return remote(part, part, bu_s.at[zz], b_r.at[zz], above)

    def early_down(zz):
        part = early_part(zz, 1 - y)
        return remote(part, part, bd_s.at[zz], b_r.at[zz], below)

    def late_a(zz, side=y):
        part = W.at[zz * PAIR + side, early:split, :]
        return remote(part, part, la_s.at[zz], la_r.at[zz], buddy)

    def late_b(zz, side=y):
        part = W.at[zz * PAIR + side, split:, :]
        return remote(part, part, lb_s.at[zz], lb_r.at[zz], buddy)

    def passed(zz, go_up, go_down):
        @pl.when((zz <= z) & has_above)
        def _():
            go_up(zz)

        @pl.when((zz >= z) & has_below)
        def _():
            go_down(zz)

    def at_distance(d, body):
        if d == 0:
            body(z)
        else:
            pl.when(z >= d)(lambda: body(z - d))
            pl.when(z + d < Z)(lambda: body(z + d))

    loads[0].wait()
    passed(z, lambda zz: up(zz).start(), lambda zz: down(zz).start())
    loads[1].wait()
    cy = [
        remote(
            C.at[rows(me), block(k * PAIR + 1 - y)], Cp.at[rows(me), pl.ds(k * B, B)],
            cy_s.at[k], cy_r.at[k], buddy,
        )
        for k in range(Z)
    ]
    for copy in cy:
        copy.start()
    early_across().start()

    def c_copy(t, f, source):
        part = C.at[rows(source), block(f)]
        return remote(part, part, c_s.at[t * fs + f], c_r.at[source * fs + f], {"tp": t})

    def c_send(side):
        for k in range(Z):
            for t in others_t:
                c_copy(t, k * PAIR + side, me).start()

    def c_wait(side):
        for k in range(Z):
            for t in others_t:
                c_copy(t, k * PAIR + side, t).wait_recv()

    def cp_copy(t, source):
        part = Cp.at[rows(source), :]
        return remote(part, part, cp_s.at[t], cp_r.at[source], {"tp": t})

    c_send(y)

    loads[2].wait()
    loads[3].wait()
    swaps = []
    for q, (a, b) in enumerate(parts):
        @pl.loop(0, T // 128)
        def _(i):
            at = pl.ds(pl.multiple_of(i * 128, 128), 128)
            g = eg[at, a:b].astype(F32)
            h = g * jax.nn.sigmoid(g) * eu[at, a:b].astype(F32)
            He[0, a:b, at] = h.T.astype(BF16)

        swaps.append(remote(He.at[0, a:b, :], He.at[1, a:b, :], h_s.at[q], h_r.at[q], buddy))
        swaps[-1].start()
    late_a(z).start()

    for copy in cy:
        copy.wait_recv()
    for t in others_t:
        cp_copy(t, me).start()
    c_send(1 - y)

    loads[4].wait()
    loads[5].wait()

    @pl.loop(0, T // 32)
    def _(i):
        at = pl.ds(pl.multiple_of(i * 32, 32), 32)
        g = lg[at, :].astype(F32)
        Hl[at, :] = (g * jax.nn.sigmoid(g) * lu[at, :].astype(F32)).astype(BF16)

    def early_relay(zz):
        part = early_part(zz, 1 - y)
        remote(part, part, by_s.at[0], b_r.at[zz], buddy).wait_recv()
        passed(zz, lambda k: early_up(k).start(), lambda k: early_down(k).start())

    def relay(zz):
        f = zz * PAIR + y
        remote(W.at[f], W.at[f], wu_s.at[zz], w_r.at[zz], buddy).wait_recv()
        passed(zz, lambda k: up(k).start(), lambda k: down(k).start())
        late_a(zz).start()

    def m_copy(f, t):
        return remote(
            Ms.at[rows(t), block(f)], Mr.at[me, :, block(f)],
            m_s.at[f * n + t], m_r.at[f * n + me], {"tp": t},
        )

    def mix(f):
        Ms[:, block(f)] = jnp.dot(Hl[...], W[f], preferred_element_type=F32).astype(BF16)
        for t in others_t:
            m_copy(f, t).start()

    def mixed_sum(f):
        for t in others_t:
            remote(
                Ms.at[rows(t), block(f)], Mr.at[t, :, block(f)],
                m_s.at[f * n + t], m_r.at[f * n + t], {"tp": t},
            ).wait_recv()
        total = Ms[rows(me), block(f)].astype(F32)
        for t in others_t:
            total = total + Mr[t, :, block(f)].astype(F32)
        mixed_ref[:, block(f)] = total.astype(BF16)

    def back(f, a, b, first=False):
        for lo, hi in cuts_of(a, b):
            term = lax.dot_general(
                C[:, block(f)], W[f, lo:hi, :], (((1,), (1,)), ((), ())),
                preferred_element_type=F32,
            )
            hc[:, lo:hi] = term if first else hc[:, lo:hi] + term

    def g_slot(zz, step):
        return jnp.where((step < 0) & (zz == z + step), Z, zz)

    def g_copy(q, zz, step):
        a, b = parts[q]
        slot = g_slot(zz, step)
        return remote(
            Gs.at[zz, a:b, :], Gr.at[slot, a:b, :],
            g_s.at[q * Z + zz], g_r.at[q * (Z + 1) + slot], {"fs": (z + step) * PAIR + y},
        )

    def g_wait(q, slot):
        a, b = parts[q]
        part = Gr.at[slot, a:b, :]
        remote(part, part, g_s.at[0], g_r.at[q * (Z + 1) + slot], buddy).wait_recv()

    def term(q, zz):
        a, b = parts[q]
        return jnp.dot(
            He[0, a:b, :], C[:, block(zz * PAIR + y)], preferred_element_type=F32
        ) + jnp.dot(He[1, a:b, :], Cp[:, block(zz)], preferred_element_type=F32)

    def each_target(body):
        @pl.loop(0, 2 * (Z - 1))
        def _(k):
            step = 1 - 2 * (k % 2)
            zz = z + step * (Z - 1 - k // 2)

            @pl.when((zz >= 0) & (zz < Z))
            def _():
                body(zz, step)

    def grad(q):
        swaps[q].wait_recv()
        a, b = parts[q]

        def onward(zz, step):
            more = jnp.where(step > 0, z > 0, z < Z - 1)

            @pl.when(more)
            def _():
                g_wait(q, zz)

            before = jnp.where(more, Gr[zz, a:b, :].astype(F32), 0.0)
            Gs[zz, a:b, :] = (term(q, zz) + before).astype(BF16)
            g_copy(q, zz, step).start()

        each_target(onward)
        if q == 0:
            loads[6].wait()
        gt_ref[a:b, :] = gt_ref[a:b, :] + term(q, z)

    def grad_end(q):
        a, b = parts[q]

        def add(slot):
            g_wait(q, slot)
            gt_ref[a:b, :] = gt_ref[a:b, :] + Gr[slot, a:b, :].astype(F32)

        pl.when(has_below)(lambda: add(z))
        pl.when(has_above)(lambda: add(Z))

    def finish(a, b):
        @pl.loop(0, T // 32)
        def _(i):
            at = pl.ds(pl.multiple_of(i * 32, 32), 32)
            g, u, h = eg[at, a:b].astype(F32), eu[at, a:b].astype(F32), hc[at, a:b]
            s = jax.nn.sigmoid(g)
            gg_ref[at, a:b] = (h * u * s * (1.0 + g * (1.0 - s))).astype(BF16)
            ug_ref[at, a:b] = (h * g * s).astype(BF16)

    def own(zz):
        return zz * PAIR + y

    def other(zz):
        return zz * PAIR + 1 - y

    early_relay(z)
    mix(own(z))
    todo = list(range(len(parts)))

    def grads(count):
        for q in todo[:count]:
            grad(q)
        del todo[:count]

    for d in range(1, Z):
        at_distance(d, relay)
        if d == Z - 1:
            for k in range(Z):
                at_distance(k, lambda zz: late_b(zz).start())
        at_distance(d, lambda zz: mix(own(zz)))
        if d == 1:
            c_wait(y)
            back(own(z), 0, K, True)
            at_distance(d, early_relay)
            at_distance(d, lambda zz: back(own(zz), 0, K))
            for t in others_t:
                cp_copy(t, t).wait_recv()
            grads(1)
        elif d < Z - 1:
            at_distance(d, lambda zz: back(own(zz), 0, K))
            grads(1)
            at_distance(d, early_relay)
            grads(len(todo) - 1 if d == Z - 2 else 1)
        else:
            at_distance(d, lambda zz: back(own(zz), 0, K))
            grads(len(todo))
            c_wait(1 - y)
            for k in range(d):
                at_distance(k, lambda zz: back(other(zz), 0, ready))
            at_distance(d, early_relay)
            at_distance(d, lambda zz: back(other(zz), 0, ready))

    def got_a(zz):
        late_a(zz, 1 - y).wait_recv()
        back(other(zz), ready, split)

    for d in range(Z):
        at_distance(d, got_a)
    finish(0, split)
    for d in range(Z):
        at_distance(d, lambda zz: mixed_sum(own(zz)))

    def got_b(zz):
        late_b(zz, 1 - y).wait_recv()
        mix(other(zz))
        back(other(zz), split, K)

    for d in range(Z):
        at_distance(d, got_b)
    finish(split, K)
    for q in range(len(parts)):
        grad_end(q)
    for d in range(Z):
        at_distance(d, lambda zz: mixed_sum(other(zz)))

    for d in range(Z):
        def sent(zz):
            passed(zz, lambda k: up(k).wait_send(), lambda k: down(k).wait_send())
            passed(zz, lambda k: early_up(k).wait_send(), lambda k: early_down(k).wait_send())
            late_a(zz).wait_send()
            late_b(zz).wait_send()

        at_distance(d, sent)
    early_across().wait_send()
    for copy in cy:
        copy.wait_send()
    for t in others_t:
        @pl.loop(0, fs)
        def _(f):
            c_copy(t, f, me).wait_send()
            m_copy(f, t).wait_send()

        cp_copy(t, me).wait_send()
    for copy in swaps:
        copy.wait_send()
    for q in range(len(parts)):
        each_target(lambda zz, step: g_copy(q, zz, step).wait_send())


def by_kernel(fs, n, *args):
    later_gate, cot, weight = args[0], args[4], args[5]
    T, K = later_gate.shape
    R, D = cot.shape
    B = weight.shape[1]
    Z = fs // PAIR
    parts = len(cuts_of(0, K))
    sem = pltpu.SemaphoreType.DMA
    anywhere = pl.BlockSpec(memory_space=pl.ANY)
    return pl.pallas_call(
        functools.partial(kernel, fs, n),
        out_shape=(
            pltpu.VMEM((R, D), BF16),
            pltpu.VMEM((T, K), BF16),
            pltpu.VMEM((T, K), BF16),
            pltpu.VMEM((K, B), F32),
        ),
        in_specs=[anywhere] * 7,
        out_specs=(pl.BlockSpec(memory_space=pltpu.VMEM),) * 4,
        scratch_shapes=[
            pltpu.VMEM((T, K), BF16), pltpu.VMEM((T, K), BF16),
            pltpu.VMEM((T, K), BF16), pltpu.VMEM((T, K), BF16),
            pltpu.VMEM((fs, K, B), BF16),
            pltpu.VMEM((T, D), BF16),
            pltpu.VMEM((T, Z * B), BF16),
            pltpu.VMEM((2, K, T), BF16),
            pltpu.VMEM((T, K), BF16),
            pltpu.VMEM((Z, K, B), BF16), pltpu.VMEM((Z + 1, K, B), BF16),
            pltpu.VMEM((T, D), BF16),
            pltpu.VMEM((n, R, D), BF16),
            pltpu.VMEM((T, K), F32),
            sem((7,)),
            sem((Z,)), sem((Z,)), sem((Z,)), sem((Z,)), sem((Z,)), sem((1,)), sem((Z,)),
            sem((Z,)), sem((Z,)), sem((Z,)), sem((Z,)),
            sem((n * fs,)), sem((n * fs,)), sem((Z,)), sem((Z,)), sem((n,)), sem((n,)),
            sem((parts,)), sem((parts,)), sem((parts * Z,)), sem((parts * (Z + 1),)),
            sem((fs * n,)), sem((fs * n,)),
        ],
        compiler_params=pltpu.CompilerParams(
            collective_id=0, has_side_effects=True, vmem_limit_bytes=52 * 2**20
        ),
    )(*args)


def solution(mesh):
    fs, n = mesh.shape["fs"], mesh.shape["tp"]

    def on_device(*args):
        T, K = args[0].shape
        B = args[5].shape[1]
        if (
            fs % PAIR == 0 and fs >= 3 * PAIR and n > 1 and B % 128 == 0 and K % 128 == 0
            and T % 128 == 0 and (T // n) % 32 == 0
        ):
            return by_kernel(fs, n, *args)
        return by_collectives(*args)

    placed = (
        P("fs", "tp"),
        P("fs", "tp"),
        P("fs", "tp"),
        P("fs", "tp"),
        P(("fs", "tp"), None),
        P("tp", "fs"),
        P("tp", "fs"),
    )
    return jax.shard_map(
        on_device,
        mesh=mesh,
        in_specs=placed,
        out_specs=(P(("fs", "tp"), None), P("fs", "tp"), P("fs", "tp"), P("tp", "fs")),
        check_vma=False,
    )
```

```python
import functools

import jax
import jax.numpy as jnp
from jax import lax
from jax.experimental import pallas as pl
from jax.experimental.pallas import tpu as pltpu
from jax.sharding import PartitionSpec as P

PAIR = 2
F32, BF16 = jnp.float32, jnp.bfloat16


def by_collectives(
    later_gate, later_up, early_gate, early_up, early_cotangent, down_weight, grad_running
):
    later_hidden = (
        jax.nn.silu(later_gate.astype(F32)) * later_up.astype(F32)
    ).astype(BF16)
    gate_value = early_gate.astype(F32)
    up_value = early_up.astype(F32)
    sigma = jax.nn.sigmoid(gate_value)
    early_hidden = (gate_value * sigma * up_value).astype(BF16)
    cot_rows = lax.all_gather(early_cotangent, "tp", axis=0, tiled=True)
    whole = lax.all_gather(down_weight, "fs", axis=1, tiled=True)
    mixed = lax.psum_scatter(
        jnp.dot(later_hidden, whole, preferred_element_type=F32).astype(BF16),
        "tp",
        scatter_dimension=0,
        tiled=True,
    )
    hidden_cot = lax.dot_general(
        cot_rows, whole, (((1,), (1,)), ((), ())), preferred_element_type=F32
    )
    gate_grad = (hidden_cot * up_value * sigma * (1.0 + gate_value * (1.0 - sigma))).astype(BF16)
    up_grad = (hidden_cot * gate_value * sigma).astype(BF16)
    summed = lax.psum_scatter(
        lax.dot_general(
            cot_rows, early_hidden, (((0,), (0,)), ((), ())), preferred_element_type=F32
        ),
        "fs",
        scatter_dimension=0,
        tiled=True,
    )
    return (mixed, gate_grad, up_grad, grad_running + summed.T)


def cuts_of(a, b, size=256):
    return [(k, min(k + size, b)) for k in range(a, b, size)]


def kernel(
    fs, n,
    lg_ref, lu_ref, eg_ref, eu_ref, cot_ref, w_ref, gr_ref,
    mixed_ref, gg_ref, ug_ref, gt_ref,
    lg, lu, eg, eu, W, C, Cp, He, Hl, Gs, Gr, Ms, Mr, hc,
    loc, wu_s, wd_s, w_r, bu_s, bd_s, by_s, b_r, l_s, l_r,
    c_s, c_r, cy_s, cy_r, cp_s, cp_r, h_s, h_r, g_s, g_r, m_s, m_r,
):
    Z = fs // PAIR
    T, K = lg.shape
    B = W.shape[2]
    R = T // n
    early = max(K // 2 // 64, 1) * 64
    ready = early // 256 * 256
    parts = cuts_of(0, K)
    last = len(parts)
    me_f, me = lax.axis_index("fs"), lax.axis_index("tp")
    z, y = me_f // PAIR, me_f % PAIR
    buddy = {"fs": z * PAIR + 1 - y}
    above, below = {"fs": (z + 1) * PAIR + y}, {"fs": (z - 1) * PAIR + y}
    has_above, has_below = z < Z - 1, z > 0

    def remote(src, dst, ss, rs, to):
        return pltpu.make_async_remote_copy(
            src_ref=src, dst_ref=dst, send_sem=ss, recv_sem=rs,
            device_id=to, device_id_type=pl.DeviceIdType.MESH,
        )

    def all_sent(part, sem):
        remote(part, part, sem.at[0], sem.at[0], buddy).wait_send()

    def all_here(part, sem):
        remote(part, part, sem, sem, buddy).wait_recv()

    def block(f):
        return pl.ds(pl.multiple_of(f * B, B), B)

    def rows(t):
        return pl.ds(pl.multiple_of(t * R, R), R)

    others_t = [lax.rem(me + k, n) for k in range(1, n)]

    loads = [
        pltpu.make_async_copy(src, dst, loc.at[i])
        for i, (src, dst) in enumerate((
            (w_ref, W.at[me_f]), (cot_ref, C.at[rows(me), :]), (eg_ref, eg), (eu_ref, eu),
            (lg_ref, lg), (lu_ref, lu), (gr_ref, gt_ref),
        ))
    ]
    for copy in loads:
        copy.start()

    barrier = pltpu.get_barrier_semaphore()

    def greet(to):
        pl.semaphore_signal(barrier, inc=1, device_id=to, device_id_type=pl.DeviceIdType.MESH)

    pl.when(has_above)(lambda: greet(above))
    pl.when(has_below)(lambda: greet(below))
    for to in [buddy] + [{"tp": t} for t in others_t]:
        greet(to)
    pl.semaphore_wait(barrier, n + has_above.astype(jnp.int32) + has_below.astype(jnp.int32))

    def up(zz):
        f = zz * PAIR + y
        return remote(W.at[f], W.at[f], wu_s.at[zz], w_r.at[zz], above)

    def down(zz):
        f = zz * PAIR + y
        return remote(W.at[f], W.at[f], wd_s.at[zz], w_r.at[zz], below)

    def early_part(zz, side):
        return W.at[zz * PAIR + side, :early, :]

    def early_across():
        part = early_part(z, y)
        return remote(part, part, by_s.at[0], b_r.at[z], buddy)

    def early_up(zz):
        part = early_part(zz, 1 - y)
        return remote(part, part, bu_s.at[zz], b_r.at[zz], above)

    def early_down(zz):
        part = early_part(zz, 1 - y)
        return remote(part, part, bd_s.at[zz], b_r.at[zz], below)

    def late(zz, lo, hi, side=y):
        part = W.at[zz * PAIR + side, early:, lo:hi]
        return remote(part, part, l_s.at[0], l_r.at[zz * 2 + lo // (B // 2)], buddy)

    def late_start(zz, d):
        for lo, hi in cut(d):
            late(zz, lo, hi).start()

    def cut(d):
        return whole if d < 2 else halves

    whole, halves = [(0, B)], [(0, B // 2), (B // 2, B)]

    def passed(zz, go_up, go_down):
        @pl.when((zz <= z) & has_above)
        def _():
            go_up(zz)

        @pl.when((zz >= z) & has_below)
        def _():
            go_down(zz)

    def at_distance(d, body):
        if d == 0:
            body(z)
        else:
            pl.when(z >= d)(lambda: body(z - d))
            pl.when(z + d < Z)(lambda: body(z + d))

    loads[0].wait()
    passed(z, lambda zz: up(zz).start(), lambda zz: down(zz).start())
    loads[1].wait()
    by_need = [jnp.where(2 * z < Z, Z - 1 - k, k) for k in range(Z)]
    cy = [
        remote(
            C.at[rows(me), block(k * PAIR + 1 - y)], Cp.at[rows(me), block(k)],
            cy_s.at[0], cy_r.at[k], buddy,
        )
        for k in by_need
    ]
    for copy in cy:
        copy.start()
    early_across().start()

    def c_copy(t, f, source):
        part = C.at[rows(source), block(f)]
        return remote(part, part, c_s.at[0], c_r.at[f % PAIR], {"tp": t})

    def c_send(side):
        for k in by_need:
            for t in others_t:
                c_copy(t, k * PAIR + side, me).start()

    def c_wait(side):
        all_here(Mr.at[: n - 1, :, : Z * B], c_r.at[side])

    def cp_copy(t, k, source):
        part = Cp.at[rows(source), block(k)]
        return remote(part, part, cp_s.at[0], cp_r.at[k], {"tp": t})

    def cp_wait(k):
        all_here(Mr.at[: n - 1, :, :B], cp_r.at[k])

    c_send(y)

    loads[2].wait()
    loads[3].wait()
    swaps = []
    for q, (a, b) in enumerate(parts):
        @pl.loop(0, T // 128)
        def _(i):
            at = pl.ds(pl.multiple_of(i * 128, 128), 128)
            g = eg[at, a:b].astype(F32)
            h = g * jax.nn.sigmoid(g) * eu[at, a:b].astype(F32)
            He[0, a:b, at] = h.T.astype(BF16)

        swaps.append(remote(He.at[0, a:b, :], He.at[1, a:b, :], h_s.at[0], h_r.at[q], buddy))
        swaps[-1].start()
    late_start(z, 0)

    for k, copy in zip(by_need, cy):
        copy.wait_recv()
        for t in others_t:
            cp_copy(t, k, me).start()
    c_send(1 - y)

    loads[4].wait()
    loads[5].wait()

    @pl.loop(0, T // 32)
    def _(i):
        at = pl.ds(pl.multiple_of(i * 32, 32), 32)
        g = lg[at, :].astype(F32)
        Hl[at, :] = (g * jax.nn.sigmoid(g) * lu[at, :].astype(F32)).astype(BF16)

    def early_relay(zz):
        part = early_part(zz, 1 - y)
        remote(part, part, by_s.at[0], b_r.at[zz], buddy).wait_recv()
        passed(zz, lambda k: early_up(k).start(), lambda k: early_down(k).start())

    def relay(d):
        def body(zz):
            f = zz * PAIR + y
            remote(W.at[f], W.at[f], wu_s.at[zz], w_r.at[zz], buddy).wait_recv()
            passed(zz, lambda k: up(k).start(), lambda k: down(k).start())
            late_start(zz, d)

        at_distance(d, body)

    def columns(f, lo, hi):
        return pl.ds(pl.multiple_of(f * B + lo, B // 2), hi - lo)

    def m_copy(f, t, lo, hi, source):
        at, i = columns(f, lo, hi), f * 2 + lo // (B // 2)
        return remote(
            Ms.at[rows(t), at], Mr.at[source, :, at],
            m_s.at[0], m_r.at[i], {"tp": t},
        )

    def mix(f, lo=0, hi=B):
        Ms[:, columns(f, lo, hi)] = jnp.dot(
            Hl[...], W[f, :, lo:hi], preferred_element_type=F32
        ).astype(BF16)
        for t in others_t:
            m_copy(f, t, lo, hi, me).start()

    def mixed_sum(f, lo=0, hi=B):
        at = columns(f, lo, hi)
        all_here(Mr.at[: n - 1, :, lo:hi], m_r.at[f * 2 + lo // (B // 2)])
        total = Ms[rows(me), at].astype(F32)
        for t in others_t:
            total = total + Mr[t, :, at].astype(F32)
        mixed_ref[:, at] = total.astype(BF16)

    def back(f, a, b, first=False):
        for lo, hi in cuts_of(a, b):
            term = lax.dot_general(
                C[:, block(f)], W[f, lo:hi, :], (((1,), (1,)), ((), ())),
                preferred_element_type=F32,
            )
            hc[:, lo:hi] = term if first else hc[:, lo:hi] + term

    def g_slot(zz, step):
        return jnp.where((step < 0) & (zz == z + step), Z, zz)

    def g_copy(q, zz, step):
        a, b = parts[q]
        slot = g_slot(zz, step)
        return remote(
            Gs.at[zz, a:b, :], Gr.at[slot, a:b, :],
            g_s.at[0], g_r.at[q * (Z + 1) + slot], {"fs": (z + step) * PAIR + y},
        )

    def g_wait(q, slot):
        a, b = parts[q]
        part = Gr.at[slot, a:b, :]
        remote(part, part, g_s.at[0], g_r.at[q * (Z + 1) + slot], buddy).wait_recv()

    def term(q, zz):
        a, b = parts[q]
        return jnp.dot(
            He[0, a:b, :], C[:, block(zz * PAIR + y)], preferred_element_type=F32
        ) + jnp.dot(He[1, a:b, :], Cp[:, block(zz)], preferred_element_type=F32)

    def each_target(body):
        @pl.loop(0, 2 * (Z - 1))
        def _(k):
            step = 1 - 2 * (k % 2)
            zz = z + step * (Z - 1 - k // 2)

            @pl.when((zz >= 0) & (zz < Z))
            def _():
                body(zz, step)

    def grad_own(q):
        a, b = parts[q]
        if q == 0:
            loads[6].wait()
        gt_ref[a:b, :] = gt_ref[a:b, :] + term(q, z)

    def grad_leaf(q):
        a, b = parts[q]

        def onward(zz, step):
            if q == 0:
                cp_wait(zz)
            Gs[zz, a:b, :] = term(q, zz).astype(BF16)
            g_copy(q, zz, step).start()

        @pl.when((z == 0) | (z == Z - 1))
        def _():
            swaps[q].wait_recv()
            each_target(onward)
            if q == 1:
                cp_wait(z)
                grad_own(0)
            if q > 0:
                grad_own(q)

    def grad_mid(slot):
        def hop(q, lag):
            a, b = parts[q]

            def onward(zz, step):
                @pl.when(jnp.where(step > 0, z, Z - 1 - z) == lag + 1)
                def _():
                    g_wait(q, zz)
                    total = term(q, zz) + Gr[zz, a:b, :].astype(F32)
                    Gs[zz, a:b, :] = total.astype(BF16)
                    g_copy(q, zz, step).start()

            each_target(onward)

        @pl.when((z > 0) & (z < Z - 1))
        def _():
            if slot == 0:
                for k in range(Z):
                    cp_wait(k)
            if slot < last:
                swaps[slot].wait_recv()
            for lag in range(Z - 2):
                if 0 <= slot - 2 * lag < last:
                    hop(slot - 2 * lag, lag)
            if slot < last:
                grad_own(slot)

    def grad_end(q):
        a, b = parts[q]

        def add(slot):
            g_wait(q, slot)
            gt_ref[a:b, :] = gt_ref[a:b, :] + Gr[slot, a:b, :].astype(F32)

        pl.when(has_below)(lambda: add(z))
        pl.when(has_above)(lambda: add(Z))

    def finish(a, b):
        @pl.loop(0, T // 32)
        def _(i):
            at = pl.ds(pl.multiple_of(i * 32, 32), 32)
            g, u, h = eg[at, a:b].astype(F32), eu[at, a:b].astype(F32), hc[at, a:b]
            s = jax.nn.sigmoid(g)
            gg_ref[at, a:b] = (h * u * s * (1.0 + g * (1.0 - s))).astype(BF16)
            ug_ref[at, a:b] = (h * g * s).astype(BF16)

    def own(zz):
        return zz * PAIR + y

    def other(zz):
        return zz * PAIR + 1 - y

    def leaf(a, b):
        for q in range(a, min(b, last)):
            grad_leaf(q)

    slots = last + 2 * (Z - 3)

    def mid(a, b):
        for slot in range(a, min(b, slots)):
            grad_mid(slot)

    def got(zz, lo, hi):
        late(zz, lo, hi, 1 - y).wait_recv()
        mix(other(zz), lo, hi)
        if hi == B:
            back(other(zz), ready, K)

    early_relay(z)
    mix(own(z))
    relay(1)
    at_distance(1, lambda zz: mix(own(zz)))
    c_wait(y)
    back(own(z), 0, K, True)
    leaf(0, 1)
    at_distance(1, early_relay)
    at_distance(1, lambda zz: back(own(zz), 0, K))
    leaf(1, 3)
    mid(0, 2)
    for d in range(2, Z - 1):
        relay(d)
        at_distance(d, lambda zz: mix(own(zz)))
        at_distance(d, lambda zz: back(own(zz), 0, K))
        leaf(d + 1, d + 2)
        at_distance(d, early_relay)
    leaf(Z, last)
    c_wait(1 - y)
    for d in range(Z - 1):
        at_distance(d, lambda zz: back(other(zz), 0, ready))
    mid(2, 3)
    relay(Z - 1)
    at_distance(Z - 1, lambda zz: mix(own(zz)))
    at_distance(Z - 1, lambda zz: back(own(zz), 0, K))
    mid(3, 4)
    got(z, 0, B)
    mid(4, 6)
    pl.when(has_below)(lambda: got(z - 1, 0, B))
    mid(6, slots - 1)
    pl.when(has_above)(lambda: got(z + 1, 0, B))
    mid(slots - 1, slots)
    at_distance(Z - 1, early_relay)
    at_distance(Z - 1, lambda zz: back(other(zz), 0, ready))
    finish(0, ready)
    for d in range(Z):
        at_distance(d, lambda zz: mixed_sum(own(zz)))
    early_across().wait_send()
    all_sent(Cp.at[rows(me), :], cy_s)
    all_sent(He.at[0], h_s)
    all_sent(Mr.at[: n - 1], c_s)
    all_sent(Mr.at[: n - 1, :, : Z * B], cp_s)
    for d in range(Z):
        def sent(zz):
            passed(zz, lambda k: up(k).wait_send(), lambda k: down(k).wait_send())
            passed(zz, lambda k: early_up(k).wait_send(), lambda k: early_down(k).wait_send())

        at_distance(d, sent)
    for d in range(2, Z):
        for lo, hi in cut(d):
            at_distance(d, lambda zz: got(zz, lo, hi))
    finish(ready, K)
    for q in range(last):
        grad_end(q)
    all_sent(Gs.at[: Z - 1], g_s)
    all_sent(W.at[:Z, early:, :], l_s)
    for d in range(Z):
        for lo, hi in cut(d):
            at_distance(d, lambda zz: mixed_sum(other(zz), lo, hi))
    all_sent(Mr.at[: n - 1], m_s)


def by_kernel(fs, n, *args):
    later_gate, cot, weight = args[0], args[4], args[5]
    T, K = later_gate.shape
    R, D = cot.shape
    B = weight.shape[1]
    Z = fs // PAIR
    parts = len(cuts_of(0, K))
    sem = pltpu.SemaphoreType.DMA
    anywhere = pl.BlockSpec(memory_space=pl.ANY)
    return pl.pallas_call(
        functools.partial(kernel, fs, n),
        out_shape=(
            pltpu.VMEM((R, D), BF16),
            pltpu.VMEM((T, K), BF16),
            pltpu.VMEM((T, K), BF16),
            pltpu.VMEM((K, B), F32),
        ),
        in_specs=[anywhere] * 7,
        out_specs=(pl.BlockSpec(memory_space=pltpu.VMEM),) * 4,
        scratch_shapes=[
            pltpu.VMEM((T, K), BF16), pltpu.VMEM((T, K), BF16),
            pltpu.VMEM((T, K), BF16), pltpu.VMEM((T, K), BF16),
            pltpu.VMEM((fs, K, B), BF16),
            pltpu.VMEM((T, D), BF16),
            pltpu.VMEM((T, Z * B), BF16),
            pltpu.VMEM((2, K, T), BF16),
            pltpu.VMEM((T, K), BF16),
            pltpu.VMEM((Z, K, B), BF16), pltpu.VMEM((Z + 1, K, B), BF16),
            pltpu.VMEM((T, D), BF16),
            pltpu.VMEM((n, R, D), BF16),
            pltpu.VMEM((T, K), F32),
            sem((7,)),
            sem((Z,)), sem((Z,)), sem((Z,)), sem((Z,)), sem((Z,)), sem((1,)), sem((Z,)),
            sem((1,)), sem((2 * Z,)),
            sem((1,)), sem((PAIR,)), sem((1,)), sem((Z,)), sem((1,)), sem((Z,)),
            sem((1,)), sem((parts,)), sem((1,)), sem((parts * (Z + 1),)),
            sem((1,)), sem((2 * fs,)),
        ],
        compiler_params=pltpu.CompilerParams(
            collective_id=0, has_side_effects=True, vmem_limit_bytes=52 * 2**20
        ),
    )(*args)


def solution(mesh):
    fs, n = mesh.shape["fs"], mesh.shape["tp"]

    def on_device(*args):
        T, K = args[0].shape
        B = args[5].shape[1]
        if (
            fs % PAIR == 0 and fs >= 3 * PAIR and n > 1 and B % 256 == 0 and K % 128 == 0 and K > 256
            and T % 128 == 0 and (T // n) % 32 == 0
        ):
            return by_kernel(fs, n, *args)
        return by_collectives(*args)

    placed = (
        P("fs", "tp"),
        P("fs", "tp"),
        P("fs", "tp"),
        P("fs", "tp"),
        P(("fs", "tp"), None),
        P("tp", "fs"),
        P("tp", "fs"),
    )
    return jax.shard_map(
        on_device,
        mesh=mesh,
        in_specs=placed,
        out_specs=(P(("fs", "tp"), None), P("fs", "tp"), P("fs", "tp"), P("tp", "fs")),
        check_vma=False,
    )
```

```python
import functools

import jax
import jax.numpy as jnp
from jax import lax
from jax.experimental import pallas as pl
from jax.experimental.pallas import tpu as pltpu
from jax.sharding import PartitionSpec as P

PAIR = 2
F32, BF16 = jnp.float32, jnp.bfloat16


def by_collectives(
    later_gate, later_up, early_gate, early_up, early_cotangent, down_weight, grad_running
):
    later_hidden = (
        jax.nn.silu(later_gate.astype(F32)) * later_up.astype(F32)
    ).astype(BF16)
    gate_value = early_gate.astype(F32)
    up_value = early_up.astype(F32)
    sigma = jax.nn.sigmoid(gate_value)
    early_hidden = (gate_value * sigma * up_value).astype(BF16)
    cot_rows = lax.all_gather(early_cotangent, "tp", axis=0, tiled=True)
    whole = lax.all_gather(down_weight, "fs", axis=1, tiled=True)
    mixed = lax.psum_scatter(
        jnp.dot(later_hidden, whole, preferred_element_type=F32).astype(BF16),
        "tp",
        scatter_dimension=0,
        tiled=True,
    )
    hidden_cot = lax.dot_general(
        cot_rows, whole, (((1,), (1,)), ((), ())), preferred_element_type=F32
    )
    gate_grad = (hidden_cot * up_value * sigma * (1.0 + gate_value * (1.0 - sigma))).astype(BF16)
    up_grad = (hidden_cot * gate_value * sigma).astype(BF16)
    summed = lax.psum_scatter(
        lax.dot_general(
            cot_rows, early_hidden, (((0,), (0,)), ((), ())), preferred_element_type=F32
        ),
        "fs",
        scatter_dimension=0,
        tiled=True,
    )
    return (mixed, gate_grad, up_grad, grad_running + summed.T)


def cuts_of(a, b, size=256):
    return [(k, min(k + size, b)) for k in range(a, b, size)]


def kernel(
    fs, n,
    lg_ref, lu_ref, eg_ref, eu_ref, cot_ref, w_ref, gr_ref,
    mixed_ref, gg_ref, ug_ref, gt_ref,
    lg, lu, eg, eu, W, C, Cp, He, Hl, Gs, Gr, Ms, Mr, hc,
    loc, wu_s, wd_s, w_r, bu_s, bd_s, by_s, b_r, l_s, l_r,
    c_s, c_r, cy_s, cy_r, cp_s, cp_r, h_s, h_r, g_s, g_r, m_s, m_r,
):
    Z = fs // PAIR
    T, K = lg.shape
    B = W.shape[2]
    R = T // n
    early = max(K * 45 // 88 // 16, 1) * 16
    ready = early // 256 * 256
    parts = cuts_of(0, K)
    last = len(parts)
    me_f, me = lax.axis_index("fs"), lax.axis_index("tp")
    z, y = me_f // PAIR, me_f % PAIR
    buddy = {"fs": z * PAIR + 1 - y}
    above, below = {"fs": (z + 1) * PAIR + y}, {"fs": (z - 1) * PAIR + y}
    has_above, has_below = z < Z - 1, z > 0

    def remote(src, dst, ss, rs, to):
        return pltpu.make_async_remote_copy(
            src_ref=src, dst_ref=dst, send_sem=ss, recv_sem=rs,
            device_id=to, device_id_type=pl.DeviceIdType.MESH,
        )

    def all_sent(part, sem):
        remote(part, part, sem.at[0], sem.at[0], buddy).wait_send()

    def all_here(part, sem):
        remote(part, part, sem, sem, buddy).wait_recv()

    def block(f):
        return pl.ds(pl.multiple_of(f * B, B), B)

    def rows(t):
        return pl.ds(pl.multiple_of(t * R, R), R)

    others_t = [lax.rem(me + k, n) for k in range(1, n)]

    loads = [
        pltpu.make_async_copy(src, dst, loc.at[i])
        for i, (src, dst) in enumerate((
            (w_ref, W.at[me_f]), (cot_ref, C.at[rows(me), :]), (eg_ref, eg), (eu_ref, eu),
            (lg_ref, lg), (lu_ref, lu), (gr_ref, gt_ref),
        ))
    ]
    for copy in loads:
        copy.start()

    barrier = pltpu.get_barrier_semaphore()

    def greet(to):
        pl.semaphore_signal(barrier, inc=1, device_id=to, device_id_type=pl.DeviceIdType.MESH)

    pl.when(has_above)(lambda: greet(above))
    pl.when(has_below)(lambda: greet(below))
    for to in [buddy] + [{"tp": t} for t in others_t]:
        greet(to)
    pl.semaphore_wait(barrier, n + has_above.astype(jnp.int32) + has_below.astype(jnp.int32))

    def up(zz):
        f = zz * PAIR + y
        return remote(W.at[f], W.at[f], wu_s.at[zz], w_r.at[zz], above)

    def down(zz):
        f = zz * PAIR + y
        return remote(W.at[f], W.at[f], wd_s.at[zz], w_r.at[zz], below)

    def early_part(zz, side):
        return W.at[zz * PAIR + side, :early, :]

    def early_across():
        part = early_part(z, y)
        return remote(part, part, by_s.at[0], b_r.at[z], buddy)

    def early_up(zz):
        part = early_part(zz, 1 - y)
        return remote(part, part, bu_s.at[zz], b_r.at[zz], above)

    def early_down(zz):
        part = early_part(zz, 1 - y)
        return remote(part, part, bd_s.at[zz], b_r.at[zz], below)

    def late(zz, lo, hi, side=y):
        part = W.at[zz * PAIR + side, early:, lo:hi]
        return remote(part, part, l_s.at[0], l_r.at[zz * 2 + lo // (B // 2)], buddy)

    def late_start(zz, d):
        for lo, hi in cut(d):
            late(zz, lo, hi).start()

    def cut(d):
        return whole if d < 2 else halves

    whole, halves = [(0, B)], [(0, B // 2), (B // 2, B)]

    def passed(zz, go_up, go_down):
        @pl.when((zz <= z) & has_above)
        def _():
            go_up(zz)

        @pl.when((zz >= z) & has_below)
        def _():
            go_down(zz)

    def at_distance(d, body):
        if d == 0:
            body(z)
        else:
            pl.when(z >= d)(lambda: body(z - d))
            pl.when(z + d < Z)(lambda: body(z + d))

    loads[0].wait()
    passed(z, lambda zz: up(zz).start(), lambda zz: down(zz).start())
    loads[1].wait()
    by_need = [jnp.where(2 * z < Z, Z - 1 - k, k) for k in range(Z)]
    cy = [
        remote(
            C.at[rows(me), block(k * PAIR + 1 - y)], Cp.at[rows(me), block(k)],
            cy_s.at[0], cy_r.at[k], buddy,
        )
        for k in by_need
    ]
    for copy in cy:
        copy.start()
    early_across().start()

    def c_copy(t, f, source):
        part = C.at[rows(source), block(f)]
        return remote(part, part, c_s.at[0], c_r.at[f % PAIR], {"tp": t})

    def c_send(side):
        for k in by_need:
            for t in others_t:
                c_copy(t, k * PAIR + side, me).start()

    def c_wait(side):
        all_here(Mr.at[: n - 1, :, : Z * B], c_r.at[side])

    def cp_copy(t, k, source):
        part = Cp.at[rows(source), block(k)]
        return remote(part, part, cp_s.at[0], cp_r.at[k], {"tp": t})

    def cp_wait(k):
        all_here(Mr.at[: n - 1, :, :B], cp_r.at[k])

    c_send(y)

    loads[2].wait()
    loads[3].wait()
    swaps = []
    for q, (a, b) in enumerate(parts):
        @pl.loop(0, T // 128)
        def _(i):
            at = pl.ds(pl.multiple_of(i * 128, 128), 128)
            g = eg[at, a:b].astype(F32)
            h = g * jax.nn.sigmoid(g) * eu[at, a:b].astype(F32)
            He[0, a:b, at] = h.T.astype(BF16)

        swaps.append(remote(He.at[0, a:b, :], He.at[1, a:b, :], h_s.at[0], h_r.at[q], buddy))
        swaps[-1].start()
    late_start(z, 0)

    for k, copy in zip(by_need, cy):
        copy.wait_recv()
        for t in others_t:
            cp_copy(t, k, me).start()
    c_send(1 - y)

    loads[4].wait()
    loads[5].wait()

    @pl.loop(0, T // 32)
    def _(i):
        at = pl.ds(pl.multiple_of(i * 32, 32), 32)
        g = lg[at, :].astype(F32)
        Hl[at, :] = (g * jax.nn.sigmoid(g) * lu[at, :].astype(F32)).astype(BF16)

    def early_relay(zz):
        part = early_part(zz, 1 - y)
        remote(part, part, by_s.at[0], b_r.at[zz], buddy).wait_recv()
        passed(zz, lambda k: early_up(k).start(), lambda k: early_down(k).start())

    def relay(d):
        def body(zz):
            f = zz * PAIR + y
            remote(W.at[f], W.at[f], wu_s.at[zz], w_r.at[zz], buddy).wait_recv()
            passed(zz, lambda k: up(k).start(), lambda k: down(k).start())
            late_start(zz, d)

        at_distance(d, body)

    def columns(f, lo, hi):
        return pl.ds(pl.multiple_of(f * B + lo, B // 2), hi - lo)

    def m_copy(f, t, lo, hi, source):
        at, i = columns(f, lo, hi), f * 2 + lo // (B // 2)
        return remote(
            Ms.at[rows(t), at], Mr.at[source, :, at],
            m_s.at[0], m_r.at[i], {"tp": t},
        )

    def mix(f, lo=0, hi=B):
        Ms[:, columns(f, lo, hi)] = jnp.dot(
            Hl[...], W[f, :, lo:hi], preferred_element_type=F32
        ).astype(BF16)
        for t in others_t:
            m_copy(f, t, lo, hi, me).start()

    def mixed_sum(f, lo=0, hi=B):
        at = columns(f, lo, hi)
        all_here(Mr.at[: n - 1, :, lo:hi], m_r.at[f * 2 + lo // (B // 2)])
        total = Ms[rows(me), at].astype(F32)
        for t in others_t:
            total = total + Mr[t, :, at].astype(F32)
        mixed_ref[:, at] = total.astype(BF16)

    def back(f, a, b, first=False):
        for lo, hi in cuts_of(a, b):
            term = lax.dot_general(
                C[:, block(f)], W[f, lo:hi, :], (((1,), (1,)), ((), ())),
                preferred_element_type=F32,
            )
            hc[:, lo:hi] = term if first else hc[:, lo:hi] + term

    def g_slot(zz, step):
        return jnp.where((step < 0) & (zz == z + step), Z, zz)

    def g_copy(q, zz, step):
        a, b = parts[q]
        slot = g_slot(zz, step)
        return remote(
            Gs.at[zz, a:b, :], Gr.at[slot, a:b, :],
            g_s.at[0], g_r.at[q * (Z + 1) + slot], {"fs": (z + step) * PAIR + y},
        )

    def g_wait(q, slot):
        a, b = parts[q]
        part = Gr.at[slot, a:b, :]
        remote(part, part, g_s.at[0], g_r.at[q * (Z + 1) + slot], buddy).wait_recv()

    def term(q, zz):
        a, b = parts[q]
        return jnp.dot(
            He[0, a:b, :], C[:, block(zz * PAIR + y)], preferred_element_type=F32
        ) + jnp.dot(He[1, a:b, :], Cp[:, block(zz)], preferred_element_type=F32)

    def each_target(body):
        @pl.loop(0, 2 * (Z - 1))
        def _(k):
            step = 1 - 2 * (k % 2)
            zz = z + step * (Z - 1 - k // 2)

            @pl.when((zz >= 0) & (zz < Z))
            def _():
                body(zz, step)

    def grad_own(q):
        a, b = parts[q]
        if q == 0:
            loads[6].wait()
        gt_ref[a:b, :] = gt_ref[a:b, :] + term(q, z)

    def grad_leaf(q):
        a, b = parts[q]

        def onward(zz, step):
            if q == 0:
                cp_wait(zz)
            Gs[zz, a:b, :] = term(q, zz).astype(BF16)
            g_copy(q, zz, step).start()

        @pl.when((z == 0) | (z == Z - 1))
        def _():
            swaps[q].wait_recv()
            each_target(onward)
            if q == 1:
                cp_wait(z)
                grad_own(0)
            if q > 0:
                grad_own(q)

    def grad_mid(slot):
        def hop(q, lag):
            a, b = parts[q]

            def onward(zz, step):
                @pl.when(jnp.where(step > 0, z, Z - 1 - z) == lag + 1)
                def _():
                    g_wait(q, zz)
                    total = term(q, zz) + Gr[zz, a:b, :].astype(F32)
                    Gs[zz, a:b, :] = total.astype(BF16)
                    g_copy(q, zz, step).start()

            each_target(onward)

        @pl.when((z > 0) & (z < Z - 1))
        def _():
            if slot == 0:
                for k in range(Z):
                    cp_wait(k)
            if slot < last:
                swaps[slot].wait_recv()
            for lag in range(Z - 2):
                if 0 <= slot - 2 * lag < last:
                    hop(slot - 2 * lag, lag)
            if slot < last:
                grad_own(slot)

    def grad_end(q):
        a, b = parts[q]

        def add(slot):
            g_wait(q, slot)
            gt_ref[a:b, :] = gt_ref[a:b, :] + Gr[slot, a:b, :].astype(F32)

        pl.when(has_below)(lambda: add(z))
        pl.when(has_above)(lambda: add(Z))

    def finish(a, b):
        @pl.loop(0, T // 32)
        def _(i):
            at = pl.ds(pl.multiple_of(i * 32, 32), 32)
            g, u, h = eg[at, a:b].astype(F32), eu[at, a:b].astype(F32), hc[at, a:b]
            s = jax.nn.sigmoid(g)
            gg_ref[at, a:b] = (h * u * s * (1.0 + g * (1.0 - s))).astype(BF16)
            ug_ref[at, a:b] = (h * g * s).astype(BF16)

    def own(zz):
        return zz * PAIR + y

    def other(zz):
        return zz * PAIR + 1 - y

    def leaf(a, b):
        for q in range(a, min(b, last)):
            grad_leaf(q)

    slots = last + 2 * (Z - 3)

    def mid(a, b):
        for slot in range(a, min(b, slots)):
            grad_mid(slot)

    def got(zz, lo, hi):
        late(zz, lo, hi, 1 - y).wait_recv()
        mix(other(zz), lo, hi)
        if hi == B:
            back(other(zz), ready, K)

    early_relay(z)
    mix(own(z))
    relay(1)
    at_distance(1, lambda zz: mix(own(zz)))
    c_wait(y)
    back(own(z), 0, K, True)
    leaf(0, 1)
    at_distance(1, early_relay)
    at_distance(1, lambda zz: back(own(zz), 0, K))
    leaf(1, 3)
    mid(0, 2)
    for d in range(2, Z - 1):
        relay(d)
        at_distance(d, lambda zz: mix(own(zz)))
        at_distance(d, lambda zz: back(own(zz), 0, K))
        leaf(d + 1, d + 2)
        at_distance(d, early_relay)
    leaf(Z, last)
    c_wait(1 - y)
    for d in range(Z - 1):
        at_distance(d, lambda zz: back(other(zz), 0, ready))
    mid(2, 3)
    relay(Z - 1)
    at_distance(Z - 1, lambda zz: mix(own(zz)))
    at_distance(Z - 1, lambda zz: back(own(zz), 0, K))
    mid(3, 4)
    got(z, 0, B)
    mid(4, 6)
    pl.when(has_below)(lambda: got(z - 1, 0, B))
    mid(6, slots - 1)
    pl.when(has_above)(lambda: got(z + 1, 0, B))
    mid(slots - 1, slots)
    at_distance(Z - 1, early_relay)
    at_distance(Z - 1, lambda zz: back(other(zz), 0, ready))
    finish(0, ready)
    for d in range(Z):
        at_distance(d, lambda zz: mixed_sum(own(zz)))
    early_across().wait_send()
    all_sent(Cp.at[rows(me), :], cy_s)
    all_sent(He.at[0], h_s)
    all_sent(Mr.at[: n - 1], c_s)
    all_sent(Mr.at[: n - 1, :, : Z * B], cp_s)
    for d in range(Z):
        def sent(zz):
            passed(zz, lambda k: up(k).wait_send(), lambda k: down(k).wait_send())
            passed(zz, lambda k: early_up(k).wait_send(), lambda k: early_down(k).wait_send())

        at_distance(d, sent)
    for d in range(2, Z):
        for lo, hi in cut(d):
            at_distance(d, lambda zz: got(zz, lo, hi))
    finish(ready, K)
    for q in range(last):
        grad_end(q)
    all_sent(Gs.at[: Z - 1], g_s)
    all_sent(W.at[:Z, early:, :], l_s)
    for d in range(Z):
        for lo, hi in cut(d):
            at_distance(d, lambda zz: mixed_sum(other(zz), lo, hi))
    all_sent(Mr.at[: n - 1], m_s)


def store(*refs):
    count = len(refs) // 2
    copies = [
        pltpu.make_async_copy(refs[i], refs[count + i], refs[-1].at[i]) for i in range(count)
    ]
    for copy in copies:
        copy.start()
    for copy in copies:
        copy.wait()


def to_hbm(arrays):
    return pl.pallas_call(
        store,
        out_shape=tuple(jax.ShapeDtypeStruct(a.shape, a.dtype) for a in arrays),
        in_specs=[pl.BlockSpec(memory_space=pltpu.VMEM)] * len(arrays),
        out_specs=(pl.BlockSpec(memory_space=pl.ANY),) * len(arrays),
        scratch_shapes=[pltpu.SemaphoreType.DMA((len(arrays),))],
        compiler_params=pltpu.CompilerParams(vmem_limit_bytes=2**20),
    )(*(pltpu.with_memory_space_constraint(a, pltpu.VMEM) for a in arrays))


def by_kernel(fs, n, *args):
    later_gate, cot, weight = args[0], args[4], args[5]
    T, K = later_gate.shape
    R, D = cot.shape
    B = weight.shape[1]
    Z = fs // PAIR
    parts = len(cuts_of(0, K))
    sem = pltpu.SemaphoreType.DMA
    anywhere = pl.BlockSpec(memory_space=pl.ANY)
    return to_hbm(pl.pallas_call(
        functools.partial(kernel, fs, n),
        out_shape=(
            pltpu.VMEM((R, D), BF16),
            pltpu.VMEM((T, K), BF16),
            pltpu.VMEM((T, K), BF16),
            pltpu.VMEM((K, B), F32),
        ),
        in_specs=[anywhere] * 7,
        out_specs=(pl.BlockSpec(memory_space=pltpu.VMEM),) * 4,
        scratch_shapes=[
            pltpu.VMEM((T, K), BF16), pltpu.VMEM((T, K), BF16),
            pltpu.VMEM((T, K), BF16), pltpu.VMEM((T, K), BF16),
            pltpu.VMEM((fs, K, B), BF16),
            pltpu.VMEM((T, D), BF16),
            pltpu.VMEM((T, Z * B), BF16),
            pltpu.VMEM((2, K, T), BF16),
            pltpu.VMEM((T, K), BF16),
            pltpu.VMEM((Z, K, B), BF16), pltpu.VMEM((Z + 1, K, B), BF16),
            pltpu.VMEM((T, D), BF16),
            pltpu.VMEM((n, R, D), BF16),
            pltpu.VMEM((T, K), F32),
            sem((7,)),
            sem((Z,)), sem((Z,)), sem((Z,)), sem((Z,)), sem((Z,)), sem((1,)), sem((Z,)),
            sem((1,)), sem((2 * Z,)),
            sem((1,)), sem((PAIR,)), sem((1,)), sem((Z,)), sem((1,)), sem((Z,)),
            sem((1,)), sem((parts,)), sem((1,)), sem((parts * (Z + 1),)),
            sem((1,)), sem((2 * fs,)),
        ],
        compiler_params=pltpu.CompilerParams(
            collective_id=0, has_side_effects=True, vmem_limit_bytes=52 * 2**20
        ),
    )(*args))


def solution(mesh):
    fs, n = mesh.shape["fs"], mesh.shape["tp"]

    def on_device(*args):
        T, K = args[0].shape
        B = args[5].shape[1]
        if (
            fs % PAIR == 0 and fs >= 3 * PAIR and n > 1 and B % 256 == 0 and K % 128 == 0 and K > 256
            and T % 128 == 0 and (T // n) % 32 == 0
        ):
            return by_kernel(fs, n, *args)
        return by_collectives(*args)

    placed = (
        P("fs", "tp"),
        P("fs", "tp"),
        P("fs", "tp"),
        P("fs", "tp"),
        P(("fs", "tp"), None),
        P("tp", "fs"),
        P("tp", "fs"),
    )
    return jax.shard_map(
        on_device,
        mesh=mesh,
        in_specs=placed,
        out_specs=(P(("fs", "tp"), None), P("fs", "tp"), P("fs", "tp"), P("tp", "fs")),
        check_vma=False,
    )
```

```python
import functools

import jax
import jax.numpy as jnp
from jax import lax
from jax.experimental import pallas as pl
from jax.experimental.pallas import tpu as pltpu
from jax.sharding import PartitionSpec as P

PAIR = 2
F32, BF16 = jnp.float32, jnp.bfloat16


def by_collectives(
    later_gate, later_up, early_gate, early_up, early_cotangent, down_weight, grad_running
):
    later_hidden = (
        jax.nn.silu(later_gate.astype(F32)) * later_up.astype(F32)
    ).astype(BF16)
    gate_value = early_gate.astype(F32)
    up_value = early_up.astype(F32)
    sigma = jax.nn.sigmoid(gate_value)
    early_hidden = (gate_value * sigma * up_value).astype(BF16)
    cot_rows = lax.all_gather(early_cotangent, "tp", axis=0, tiled=True)
    whole = lax.all_gather(down_weight, "fs", axis=1, tiled=True)
    mixed = lax.psum_scatter(
        jnp.dot(later_hidden, whole, preferred_element_type=F32).astype(BF16),
        "tp",
        scatter_dimension=0,
        tiled=True,
    )
    hidden_cot = lax.dot_general(
        cot_rows, whole, (((1,), (1,)), ((), ())), preferred_element_type=F32
    )
    gate_grad = (hidden_cot * up_value * sigma * (1.0 + gate_value * (1.0 - sigma))).astype(BF16)
    up_grad = (hidden_cot * gate_value * sigma).astype(BF16)
    summed = lax.psum_scatter(
        lax.dot_general(
            cot_rows, early_hidden, (((0,), (0,)), ((), ())), preferred_element_type=F32
        ),
        "fs",
        scatter_dimension=0,
        tiled=True,
    )
    return (mixed, gate_grad, up_grad, grad_running + summed.T)


def cuts_of(a, b, size=256):
    return [(k, min(k + size, b)) for k in range(a, b, size)]


def kernel(
    fs, n,
    lg_ref, lu_ref, eg_ref, eu_ref, cot_ref, w_ref, gr_ref,
    mixed_ref, gg_ref, ug_ref, gt_ref,
    lg, lu, eg, eu, W, C, Cp, He, Hl, Gs, Gr, Ms, Mr, hc, Ma,
    loc, wu_s, wd_s, w_r, bu_s, bd_s, by_s, b_r, l_s, l_r,
    c_s, c_r, cy_s, cy_r, cp_s, cp_r, h_s, h_r, g_s, g_r, m_s, m_r,
):
    Z = fs // PAIR
    T, K = lg.shape
    B = W.shape[2]
    R = T // n
    early = max(K * 45 // 88 // 16, 1) * 16
    ready = early // 256 * 256
    parts = cuts_of(0, K)
    last = len(parts)
    me_f, me = lax.axis_index("fs"), lax.axis_index("tp")
    z, y = me_f // PAIR, me_f % PAIR
    buddy = {"fs": z * PAIR + 1 - y}
    above, below = {"fs": (z + 1) * PAIR + y}, {"fs": (z - 1) * PAIR + y}
    has_above, has_below = z < Z - 1, z > 0

    def remote(src, dst, ss, rs, to):
        return pltpu.make_async_remote_copy(
            src_ref=src, dst_ref=dst, send_sem=ss, recv_sem=rs,
            device_id=to, device_id_type=pl.DeviceIdType.MESH,
        )

    def all_sent(part, sem):
        remote(part, part, sem.at[0], sem.at[0], buddy).wait_send()

    def all_here(part, sem):
        remote(part, part, sem, sem, buddy).wait_recv()

    def block(f):
        return pl.ds(pl.multiple_of(f * B, B), B)

    def rows(t):
        return pl.ds(pl.multiple_of(t * R, R), R)

    others_t = [lax.rem(me + k, n) for k in range(1, n)]

    loads = [
        pltpu.make_async_copy(src, dst, loc.at[i])
        for i, (src, dst) in enumerate((
            (w_ref, W.at[me_f]), (cot_ref, C.at[rows(me), :]), (eg_ref, eg), (eu_ref, eu),
            (lg_ref, lg), (lu_ref, lu), (gr_ref, gt_ref),
        ))
    ]
    for copy in loads:
        copy.start()

    barrier = pltpu.get_barrier_semaphore()

    def greet(to):
        pl.semaphore_signal(barrier, inc=1, device_id=to, device_id_type=pl.DeviceIdType.MESH)

    pl.when(has_above)(lambda: greet(above))
    pl.when(has_below)(lambda: greet(below))
    for to in [buddy] + [{"tp": t} for t in others_t]:
        greet(to)
    pl.semaphore_wait(barrier, n + has_above.astype(jnp.int32) + has_below.astype(jnp.int32))

    def up(zz):
        f = zz * PAIR + y
        return remote(W.at[f], W.at[f], wu_s.at[zz], w_r.at[zz], above)

    def down(zz):
        f = zz * PAIR + y
        return remote(W.at[f], W.at[f], wd_s.at[zz], w_r.at[zz], below)

    def early_part(zz, side):
        return W.at[zz * PAIR + side, :early, :]

    def early_across():
        part = early_part(z, y)
        return remote(part, part, by_s.at[0], b_r.at[z], buddy)

    def early_up(zz):
        part = early_part(zz, 1 - y)
        return remote(part, part, bu_s.at[zz], b_r.at[zz], above)

    def early_down(zz):
        part = early_part(zz, 1 - y)
        return remote(part, part, bd_s.at[zz], b_r.at[zz], below)

    def late(zz, lo, hi, side=y):
        part = W.at[zz * PAIR + side, early:, lo:hi]
        return remote(part, part, l_s.at[0], l_r.at[zz * 2 + lo // (B // 2)], buddy)

    def late_start(zz, d):
        for lo, hi in cut(d):
            late(zz, lo, hi).start()

    def cut(d):
        return whole if d < 2 else halves

    whole, halves = [(0, B)], [(0, B // 2), (B // 2, B)]

    def passed(zz, go_up, go_down):
        @pl.when((zz <= z) & has_above)
        def _():
            go_up(zz)

        @pl.when((zz >= z) & has_below)
        def _():
            go_down(zz)

    def at_distance(d, body):
        if d == 0:
            body(z)
        else:
            pl.when(z >= d)(lambda: body(z - d))
            pl.when(z + d < Z)(lambda: body(z + d))

    loads[0].wait()
    passed(z, lambda zz: up(zz).start(), lambda zz: down(zz).start())
    loads[1].wait()
    by_need = [jnp.where(2 * z < Z, Z - 1 - k, k) for k in range(Z)]
    cy = [
        remote(
            C.at[rows(me), block(k * PAIR + 1 - y)], Cp.at[rows(me), block(k)],
            cy_s.at[0], cy_r.at[k], buddy,
        )
        for k in by_need
    ]
    for copy in cy:
        copy.start()
    early_across().start()

    def c_copy(t, f, source):
        part = C.at[rows(source), block(f)]
        return remote(part, part, c_s.at[0], c_r.at[f % PAIR], {"tp": t})

    def c_send(side):
        for k in by_need:
            for t in others_t:
                c_copy(t, k * PAIR + side, me).start()

    def c_wait(side):
        all_here(Mr.at[: n - 1, :, : Z * B], c_r.at[side])

    def cp_copy(t, k, source):
        part = Cp.at[rows(source), block(k)]
        return remote(part, part, cp_s.at[0], cp_r.at[k], {"tp": t})

    def cp_wait(k):
        all_here(Mr.at[: n - 1, :, :B], cp_r.at[k])

    c_send(y)

    loads[2].wait()
    loads[3].wait()
    swaps = []
    for q, (a, b) in enumerate(parts):
        @pl.loop(0, T // 128)
        def _(i):
            at = pl.ds(pl.multiple_of(i * 128, 128), 128)
            g = eg[at, a:b].astype(F32)
            h = g * jax.nn.sigmoid(g) * eu[at, a:b].astype(F32)
            He[0, a:b, at] = h.T.astype(BF16)

        swaps.append(remote(He.at[0, a:b, :], He.at[1, a:b, :], h_s.at[0], h_r.at[q], buddy))
        swaps[-1].start()
    late_start(z, 0)

    for k, copy in zip(by_need, cy):
        copy.wait_recv()
        for t in others_t:
            cp_copy(t, k, me).start()
    c_send(1 - y)

    loads[4].wait()
    loads[5].wait()

    @pl.loop(0, T // 32)
    def _(i):
        at = pl.ds(pl.multiple_of(i * 32, 32), 32)
        g = lg[at, :].astype(F32)
        Hl[at, :] = (g * jax.nn.sigmoid(g) * lu[at, :].astype(F32)).astype(BF16)

    def early_relay(zz):
        part = early_part(zz, 1 - y)
        remote(part, part, by_s.at[0], b_r.at[zz], buddy).wait_recv()
        passed(zz, lambda k: early_up(k).start(), lambda k: early_down(k).start())

    def relay(d):
        def body(zz):
            f = zz * PAIR + y
            remote(W.at[f], W.at[f], wu_s.at[zz], w_r.at[zz], buddy).wait_recv()
            passed(zz, lambda k: up(k).start(), lambda k: down(k).start())
            late_start(zz, d)

        at_distance(d, body)

    def columns(f, lo, hi):
        return pl.ds(pl.multiple_of(f * B + lo, B // 2), hi - lo)

    def m_copy(f, t, lo, hi, source):
        at, i = columns(f, lo, hi), f * 2 + lo // (B // 2)
        return remote(
            Ms.at[rows(t), at], Mr.at[source, :, at],
            m_s.at[0], m_r.at[i], {"tp": t},
        )

    def mix(f, lo=0, hi=B, begun=None):
        if begun is None:
            total = jnp.dot(Hl[...], W[f, :, lo:hi], preferred_element_type=F32)
        else:
            total = begun + jnp.dot(
                Hl[:, ready:], W[f, ready:, lo:hi], preferred_element_type=F32
            )
        Ms[:, columns(f, lo, hi)] = total.astype(BF16)
        for t in others_t:
            m_copy(f, t, lo, hi, me).start()

    def mixed_sum(f, lo=0, hi=B):
        at = columns(f, lo, hi)
        all_here(Mr.at[: n - 1, :, lo:hi], m_r.at[f * 2 + lo // (B // 2)])
        total = Ms[rows(me), at].astype(F32)
        for t in others_t:
            total = total + Mr[t, :, at].astype(F32)
        mixed_ref[:, at] = total.astype(BF16)

    def back(f, a, b, first=False):
        for lo, hi in cuts_of(a, b):
            term = lax.dot_general(
                C[:, block(f)], W[f, lo:hi, :], (((1,), (1,)), ((), ())),
                preferred_element_type=F32,
            )
            hc[:, lo:hi] = term if first else hc[:, lo:hi] + term

    def g_slot(zz, step):
        return jnp.where((step < 0) & (zz == z + step), Z, zz)

    def g_copy(q, zz, step):
        a, b = parts[q]
        slot = g_slot(zz, step)
        return remote(
            Gs.at[zz, a:b, :], Gr.at[slot, a:b, :],
            g_s.at[0], g_r.at[q * (Z + 1) + slot], {"fs": (z + step) * PAIR + y},
        )

    def g_wait(q, slot):
        a, b = parts[q]
        part = Gr.at[slot, a:b, :]
        remote(part, part, g_s.at[0], g_r.at[q * (Z + 1) + slot], buddy).wait_recv()

    def term(q, zz):
        a, b = parts[q]
        return jnp.dot(
            He[0, a:b, :], C[:, block(zz * PAIR + y)], preferred_element_type=F32
        ) + jnp.dot(He[1, a:b, :], Cp[:, block(zz)], preferred_element_type=F32)

    def each_target(body):
        @pl.loop(0, 2 * (Z - 1))
        def _(k):
            step = 1 - 2 * (k % 2)
            zz = z + step * (Z - 1 - k // 2)

            @pl.when((zz >= 0) & (zz < Z))
            def _():
                body(zz, step)

    def grad_own(q):
        a, b = parts[q]
        if q == 0:
            loads[6].wait()
        gt_ref[a:b, :] = gt_ref[a:b, :] + term(q, z)

    def grad_leaf(q):
        a, b = parts[q]

        def onward(zz, step):
            if q == 0:
                cp_wait(zz)
            Gs[zz, a:b, :] = term(q, zz).astype(BF16)
            g_copy(q, zz, step).start()

        @pl.when((z == 0) | (z == Z - 1))
        def _():
            swaps[q].wait_recv()
            each_target(onward)
            if q == 1:
                cp_wait(z)
                grad_own(0)
            if q > 0:
                grad_own(q)

    def grad_mid(slot):
        def hop(q, lag):
            a, b = parts[q]

            def onward(zz, step):
                @pl.when(jnp.where(step > 0, z, Z - 1 - z) == lag + 1)
                def _():
                    g_wait(q, zz)
                    total = term(q, zz) + Gr[zz, a:b, :].astype(F32)
                    Gs[zz, a:b, :] = total.astype(BF16)
                    g_copy(q, zz, step).start()

            each_target(onward)

        @pl.when((z > 0) & (z < Z - 1))
        def _():
            if slot == 0:
                for k in range(Z):
                    cp_wait(k)
            if slot < last:
                swaps[slot].wait_recv()
            for lag in range(Z - 2):
                if 0 <= slot - 2 * lag < last:
                    hop(slot - 2 * lag, lag)
            if slot < last:
                grad_own(slot)

    def grad_end(q):
        a, b = parts[q]

        def add(slot):
            g_wait(q, slot)
            gt_ref[a:b, :] = gt_ref[a:b, :] + Gr[slot, a:b, :].astype(F32)

        pl.when(has_below)(lambda: add(z))
        pl.when(has_above)(lambda: add(Z))

    def finish(a, b):
        @pl.loop(0, T // 32)
        def _(i):
            at = pl.ds(pl.multiple_of(i * 32, 32), 32)
            g, u, h = eg[at, a:b].astype(F32), eu[at, a:b].astype(F32), hc[at, a:b]
            s = jax.nn.sigmoid(g)
            gg_ref[at, a:b] = (h * u * s * (1.0 + g * (1.0 - s))).astype(BF16)
            ug_ref[at, a:b] = (h * g * s).astype(BF16)

    def own(zz):
        return zz * PAIR + y

    def other(zz):
        return zz * PAIR + 1 - y

    def leaf(a, b):
        for q in range(a, min(b, last)):
            grad_leaf(q)

    slots = last + 2 * (Z - 3)

    def mid(a, b):
        for slot in range(a, min(b, slots)):
            grad_mid(slot)

    def begin(zz):
        Ma[zz] = jnp.dot(
            Hl[:, :ready], W[other(zz), :ready, :], preferred_element_type=F32
        )

    def got(zz, lo, hi, begun=False):
        late(zz, lo, hi, 1 - y).wait_recv()
        mix(other(zz), lo, hi, Ma[zz, :, lo:hi] if begun else None)
        if hi == B:
            back(other(zz), ready, K)

    early_relay(z)
    mix(own(z))
    relay(1)
    at_distance(1, lambda zz: mix(own(zz)))
    c_wait(y)
    back(own(z), 0, K, True)
    leaf(0, 1)
    at_distance(1, early_relay)
    at_distance(1, lambda zz: back(own(zz), 0, K))
    leaf(1, 3)
    mid(0, 2)
    for d in range(2, Z - 1):
        relay(d)
        at_distance(d, lambda zz: mix(own(zz)))
        at_distance(d, lambda zz: back(own(zz), 0, K))
        leaf(d + 1, d + 2)
        at_distance(d, early_relay)
    leaf(Z, last)
    c_wait(1 - y)
    for d in range(Z - 1):
        at_distance(d, lambda zz: back(other(zz), 0, ready))
    mid(2, 3)
    relay(Z - 1)
    at_distance(Z - 1, lambda zz: mix(own(zz)))
    at_distance(Z - 1, lambda zz: back(own(zz), 0, K))
    mid(3, 4)
    got(z, 0, B)
    mid(4, 6)
    pl.when(has_below)(lambda: got(z - 1, 0, B))
    mid(6, slots - 1)
    pl.when(has_above)(lambda: got(z + 1, 0, B))
    mid(slots - 1, slots)
    at_distance(Z - 1, early_relay)
    at_distance(Z - 1, lambda zz: back(other(zz), 0, ready))
    finish(0, ready)
    for d in range(2, Z):
        at_distance(d, begin)
    for d in range(Z):
        at_distance(d, lambda zz: mixed_sum(own(zz)))
    early_across().wait_send()
    all_sent(Cp.at[rows(me), :], cy_s)
    all_sent(He.at[0], h_s)
    all_sent(Mr.at[: n - 1], c_s)
    all_sent(Mr.at[: n - 1, :, : Z * B], cp_s)
    for d in range(Z):
        def sent(zz):
            passed(zz, lambda k: up(k).wait_send(), lambda k: down(k).wait_send())
            passed(zz, lambda k: early_up(k).wait_send(), lambda k: early_down(k).wait_send())

        at_distance(d, sent)
    for d in range(2, Z):
        for lo, hi in cut(d):
            at_distance(d, lambda zz: got(zz, lo, hi, True))
    finish(ready, K)
    for q in range(last):
        grad_end(q)
    all_sent(Gs.at[: Z - 1], g_s)
    all_sent(W.at[:Z, early:, :], l_s)
    for d in range(Z):
        for lo, hi in cut(d):
            at_distance(d, lambda zz: mixed_sum(other(zz), lo, hi))
    all_sent(Mr.at[: n - 1], m_s)


def store(*refs):
    count = len(refs) // 2
    copies = [
        pltpu.make_async_copy(refs[i], refs[count + i], refs[-1].at[i]) for i in range(count)
    ]
    for copy in copies:
        copy.start()
    for copy in copies:
        copy.wait()


def to_hbm(arrays):
    return pl.pallas_call(
        store,
        out_shape=tuple(jax.ShapeDtypeStruct(a.shape, a.dtype) for a in arrays),
        in_specs=[pl.BlockSpec(memory_space=pltpu.VMEM)] * len(arrays),
        out_specs=(pl.BlockSpec(memory_space=pl.ANY),) * len(arrays),
        scratch_shapes=[pltpu.SemaphoreType.DMA((len(arrays),))],
        compiler_params=pltpu.CompilerParams(vmem_limit_bytes=2**20),
    )(*(pltpu.with_memory_space_constraint(a, pltpu.VMEM) for a in arrays))


def by_kernel(fs, n, *args):
    later_gate, cot, weight = args[0], args[4], args[5]
    T, K = later_gate.shape
    R, D = cot.shape
    B = weight.shape[1]
    Z = fs // PAIR
    parts = len(cuts_of(0, K))
    sem = pltpu.SemaphoreType.DMA
    anywhere = pl.BlockSpec(memory_space=pl.ANY)
    return to_hbm(pl.pallas_call(
        functools.partial(kernel, fs, n),
        out_shape=(
            pltpu.VMEM((R, D), BF16),
            pltpu.VMEM((T, K), BF16),
            pltpu.VMEM((T, K), BF16),
            pltpu.VMEM((K, B), F32),
        ),
        in_specs=[anywhere] * 7,
        out_specs=(pl.BlockSpec(memory_space=pltpu.VMEM),) * 4,
        scratch_shapes=[
            pltpu.VMEM((T, K), BF16), pltpu.VMEM((T, K), BF16),
            pltpu.VMEM((T, K), BF16), pltpu.VMEM((T, K), BF16),
            pltpu.VMEM((fs, K, B), BF16),
            pltpu.VMEM((T, D), BF16),
            pltpu.VMEM((T, Z * B), BF16),
            pltpu.VMEM((2, K, T), BF16),
            pltpu.VMEM((T, K), BF16),
            pltpu.VMEM((Z, K, B), BF16), pltpu.VMEM((Z + 1, K, B), BF16),
            pltpu.VMEM((T, D), BF16),
            pltpu.VMEM((n, R, D), BF16),
            pltpu.VMEM((T, K), F32),
            pltpu.VMEM((Z, T, B), F32),
            sem((7,)),
            sem((Z,)), sem((Z,)), sem((Z,)), sem((Z,)), sem((Z,)), sem((1,)), sem((Z,)),
            sem((1,)), sem((2 * Z,)),
            sem((1,)), sem((PAIR,)), sem((1,)), sem((Z,)), sem((1,)), sem((Z,)),
            sem((1,)), sem((parts,)), sem((1,)), sem((parts * (Z + 1),)),
            sem((1,)), sem((2 * fs,)),
        ],
        compiler_params=pltpu.CompilerParams(
            collective_id=0, has_side_effects=True, vmem_limit_bytes=52 * 2**20
        ),
    )(*args))


def solution(mesh):
    fs, n = mesh.shape["fs"], mesh.shape["tp"]

    def on_device(*args):
        T, K = args[0].shape
        B = args[5].shape[1]
        if (
            fs % PAIR == 0 and fs >= 3 * PAIR and n > 1 and B % 256 == 0 and K % 128 == 0 and K > 256
            and T % 128 == 0 and (T // n) % 32 == 0
        ):
            return by_kernel(fs, n, *args)
        return by_collectives(*args)

    placed = (
        P("fs", "tp"),
        P("fs", "tp"),
        P("fs", "tp"),
        P("fs", "tp"),
        P(("fs", "tp"), None),
        P("tp", "fs"),
        P("tp", "fs"),
    )
    return jax.shard_map(
        on_device,
        mesh=mesh,
        in_specs=placed,
        out_specs=(P(("fs", "tp"), None), P("fs", "tp"), P("fs", "tp"), P("tp", "fs")),
        check_vma=False,
    )
```
